1024 devices in a mesh: grp: 2 (over x), tp: 16 (over z), dp: 32 (over y, core).
Axes of the slice: x: 2, y: 16, z: 16, core: 2. Of those that a mesh axis runs over, the one named last changes fastest.
The devices are a block of a 4x16x16 slice.
Arguments:
- hidden: bfloat16 [128, 2048], P('grp', 'dp'), parts along dimension 0, may hold values from -20 to 20
- lengths: int32 [128], P(('grp', 'dp')), parts along dimension 0, may hold values from 1 to 256, 4096 in all
- input_norm_gain: float32 [2, 2048], P(None, 'dp'), may hold values from 0.1 to 1.9
- gate_matrix: bfloat16 [2, 2048, 4096], P(None, 'dp', 'tp'), may hold values from -0.125 to 0.125
- input_matrix: bfloat16 [2, 2048, 4096], P(None, 'dp', 'tp'), may hold values from -0.125 to 0.125
- write_matrix: bfloat16 [2, 2048, 2048], P(None, 'dp', 'tp'), may hold values from -0.125 to 0.125
- read_matrix: bfloat16 [2, 2048, 2048], P(None, 'dp', 'tp'), may hold values from -0.125 to 0.125
- step_matrix: bfloat16 [2, 2048, 64], P(None, 'dp'), may hold values from -0.125 to 0.125
- step_size_bias: float32 [2, 64], P(None, 'tp'), may hold values from -2 to 1
- log_decay_rate: float32 [2, 64], P(None, 'tp'), may hold values from -1 to 2
- direct_path_gain: float32 [2, 64], P(None, 'tp'), may hold values from 0.5 to 1.5
- input_filter_taps: bfloat16 [2, 4, 4096], P(None, None, 'tp'), may hold values from -3 to 3
- write_filter_taps: bfloat16 [2, 4, 2048], P(None, None, 'tp'), may hold values from -3 to 3
- read_filter_taps: bfloat16 [2, 4, 2048], P(None, None, 'tp'), may hold values from -3 to 3
- position_log_decay: float32 [2, 256, 64], P(None, None, 'tp'), may hold values from -0.7 to 0
- grouped_norm_gain: float32 [2, 4096], P(None, 'tp'), may hold values from 0.1 to 1.9
- output_matrix: bfloat16 [2, 4096, 2048], P(None, 'tp', 'dp'), may hold values from -0.09375 to 0.09375
- recurrent_head_state: float32 [2, 128, 64, 64, 128], P(None, ('grp', 'dp'), 'tp'), parts along dimension 1, may hold values from -3 to 3
- history_input_rows: bfloat16 [2, 128, 3, 4096], P(None, ('grp', 'dp'), None, 'tp'), parts along dimension 1, may hold values from -5 to 5
- history_write_rows: bfloat16 [2, 128, 3, 2048], P(None, ('grp', 'dp'), None, 'tp'), parts along dimension 1, may hold values from -5 to 5
- history_read_rows: bfloat16 [2, 128, 3, 2048], P(None, ('grp', 'dp'), None, 'tp'), parts along dimension 1, may hold values from -5 to 5
Outputs:
- stream_out: bfloat16 [128, 2048], P('grp', 'dp'), parts along dimension 0
- state_out: float32 [2, 128, 64, 64, 128], P(None, ('grp', 'dp'), 'tp'), parts along dimension 1
- buffer_value_out: bfloat16 [2, 128, 3, 4096], P(None, ('grp', 'dp'), None, 'tp'), parts along dimension 1
- buffer_write_out: bfloat16 [2, 128, 3, 2048], P(None, ('grp', 'dp'), None, 'tp'), parts along dimension 1
- buffer_read_out: bfloat16 [2, 128, 3, 2048], P(None, ('grp', 'dp'), None, 'tp'), parts along dimension 1
The draws below stay inside these ranges and needn't reach their ends.
There are 2 independent parts, one for each index of `grp`. The reference program is written for one: setup_inputs(seed, part) draws one part's arguments, and reference() takes and returns one part's arrays. A program takes and returns all parts, laid end to end along the dimension named above; an argument that names none is the same for every part. Nothing has to cross between parts.
Inputs may be any that keep to these rules, and one draw needn't show every extreme that they name: `lengths`: a sequence's current token stands at position length - 1; some sequence has length 256.
All inputs are finite; a program needn't handle non-finite values. No bound on the sum of `lengths` on one device may be relied on, other than what follows from the above.
Results may differ from the reference program's by a relative error of at most 0.0065.
Values may be sent and summed in bfloat16 or wider, within the bound.
A program may use at most 32 MiB of HBM per device.

```python
import math
import jax
import jax.numpy as jnp
import numpy as np
from jax import lax

D = 2048
MIXER_HEADS = 64
HEAD_DIM = 64
GROUPS = 16
STATE = 128
TAPS = 4
MIXER_LAYERS = 2
LONGEST_LENGTH = 256
MEAN_LEN = 64
SEQS = 64
INNER = 4096


def draw_hidden(key, part):
    base_key = jax.random.fold_in(key, 17)
    row_key, entry_key = jax.random.split(base_key, 2)
    row_scales = jnp.exp(jax.random.uniform(row_key, (SEQS, 1), jnp.float32, math.log(0.3), math.log(3.0)))
    column_scales = jnp.exp(math.log(0.6) + math.log(3.0) * jnp.arange(D, dtype=jnp.float32) / D)[None, :]
    values = jnp.clip(jax.random.normal(entry_key, (SEQS, D), jnp.float32), -3.0, 3.0)
    return (values * row_scales * column_scales).astype(jnp.bfloat16)


def levels(key, dims, shards, least, high):
    def one(position, blocks):
        heights = jax.random.uniform(jax.random.fold_in(jax.random.fold_in(key, 6), position), (blocks,), jnp.float32, least / len(shards), high / len(shards))
        return jnp.repeat(jnp.exp(heights), dims[position] // blocks).reshape((-1,) + (1,) * (len(dims) - position - 1))

    factor_of = one(*shards[0])
    for cut in shards[1:]:
        factor_of = factor_of * one(*cut)
    return factor_of


def split_up(amount, total, limit, slope):
    weights = [(1 << 20) // math.isqrt(standing ** slope) + 1 for standing in range(2, amount + 1)]
    surplus, counts = total - limit - (amount - 1), [1] * (amount - 1)
    while surplus > 0:
        movable = [i for i in range(amount - 1) if counts[i] < limit]
        whole, left = sum([weights[i] for i in movable]), surplus
        for i in movable:
            extra = min(limit - counts[i], max(1, left * weights[i] // whole), surplus)
            counts[i] = counts[i] + extra
            surplus = surplus - extra
    return np.array([limit] + counts)


def uneven(key, count, total, limit, skew):
    if count == 2:
        one = jax.random.randint(key, (), max(1, total - limit), min(limit, total - 1) + 1)
        return jnp.stack([one, total - one])
    sizes = jnp.asarray(split_up(count, total, limit, skew), jnp.int32)
    couples = (count - 1) // 2
    donor, sink = sizes[1:1 + 2 * couples:2], sizes[2:2 + 2 * couples:2]
    room = jnp.minimum(donor - 1, limit - sink)
    moved = jax.random.randint(jax.random.fold_in(key, 1), (couples,), 0, 1 << 20) % (room + 1)
    sizes = sizes.at[1:1 + 2 * couples:2].set(donor - moved).at[2:2 + 2 * couples:2].set(sink + moved)
    return sizes[jax.random.permutation(jax.random.fold_in(key, 2), count)]


def normal_values(own_key, extent, spread, reach, pieces=(), kind=jnp.bfloat16):
    level = levels(own_key, extent, pieces, -0.22, 0.18) if pieces else 1.0
    entries = jax.random.normal(own_key, extent, jnp.float32) * spread * level
    return jnp.minimum(jnp.maximum(entries, -reach), reach).astype(kind)


def setup_inputs(seed: int = 0, part: int = 0) -> dict:
    splits = jax.random.split(jax.random.key(seed), 22)
    part_splits = jax.random.split(jax.random.fold_in(splits[21], part), 22)
    hidden = draw_hidden(jax.random.fold_in(jax.random.fold_in(splits[21], part), 71), part)
    lengths = uneven(part_splits[1], SEQS, SEQS * MEAN_LEN, LONGEST_LENGTH, 2).astype(jnp.int32)
    input_norm_gain = jnp.clip(1.0 + 0.18 * jax.random.normal(splits[2], (MIXER_LAYERS, D), jnp.float32), 0.1, 1.9)
    gate_matrix = normal_values(splits[3], (MIXER_LAYERS, D, INNER), D ** -0.5, 0.125, ((1, 32), (2, 16)))
    input_matrix = normal_values(splits[4], (MIXER_LAYERS, D, INNER), D ** -0.5, 0.125, ((1, 32), (2, 16)))
    write_matrix = normal_values(splits[5], (MIXER_LAYERS, D, GROUPS * STATE), D ** -0.5, 0.125, ((1, 32), (2, 16)))
    read_matrix = normal_values(splits[6], (MIXER_LAYERS, D, GROUPS * STATE), D ** -0.5, 0.125, ((1, 32), (2, 16)))
    step_matrix = normal_values(splits[7], (MIXER_LAYERS, D, MIXER_HEADS), D ** -0.5, 0.125, ((1, 32),))
    step_size_bias = jnp.clip(-2.0 + 3.0 * jax.random.uniform(splits[8], (MIXER_LAYERS, MIXER_HEADS), jnp.float32) ** levels(splits[8], (MIXER_LAYERS, MIXER_HEADS), ((1, 16),), -0.2, 0.2), -2.0, 1.0)
    log_decay_rate = jnp.clip(-1.0 + 3.0 * jax.random.uniform(splits[9], (MIXER_LAYERS, MIXER_HEADS), jnp.float32) ** levels(splits[9], (MIXER_LAYERS, MIXER_HEADS), ((1, 16),), -0.2, 0.2), -1.0, 2.0)
    direct_path_gain = jnp.clip(0.5 + 1.0 * jax.random.uniform(splits[10], (MIXER_LAYERS, MIXER_HEADS), jnp.float32) ** levels(splits[10], (MIXER_LAYERS, MIXER_HEADS), ((1, 16),), -0.2, 0.2), 0.5, 1.5)
    input_filter_taps = normal_values(splits[11], (MIXER_LAYERS, TAPS, INNER), TAPS ** -0.5, 3.0, ((2, 16),))
    write_filter_taps = normal_values(splits[12], (MIXER_LAYERS, TAPS, GROUPS * STATE), TAPS ** -0.5, 3.0, ((2, 16),))
    read_filter_taps = normal_values(splits[13], (MIXER_LAYERS, TAPS, GROUPS * STATE), TAPS ** -0.5, 3.0, ((2, 16),))
    position_log_decay = jnp.clip(-0.7 + 0.7 * jax.random.uniform(splits[14], (MIXER_LAYERS, LONGEST_LENGTH, MIXER_HEADS), jnp.float32) ** levels(splits[14], (MIXER_LAYERS, LONGEST_LENGTH, MIXER_HEADS), ((2, 16),), -0.2, 0.2), -0.7, 0.0)
    grouped_norm_gain = jnp.clip(1.0 + 0.18 * jax.random.normal(splits[15], (MIXER_LAYERS, INNER), jnp.float32), 0.1, 1.9)
    output_matrix = normal_values(splits[16], (MIXER_LAYERS, INNER, D), INNER ** -0.5, 0.09375, ((1, 16), (2, 32)))
    recurrent_head_state = normal_values(part_splits[17], (MIXER_LAYERS, SEQS, MIXER_HEADS, HEAD_DIM, STATE), 0.5, 3.0, ((1, 32), (2, 16)), jnp.float32)
    history_input_rows = normal_values(part_splits[18], (MIXER_LAYERS, SEQS, TAPS - 1, INNER), 1.0, 5.0, ((1, 32), (3, 16)))
    history_write_rows = normal_values(part_splits[19], (MIXER_LAYERS, SEQS, TAPS - 1, GROUPS * STATE), 1.0, 5.0, ((1, 32), (3, 16)))
    history_read_rows = normal_values(part_splits[20], (MIXER_LAYERS, SEQS, TAPS - 1, GROUPS * STATE), 1.0, 5.0, ((1, 32), (3, 16)))
    return {"hidden": hidden, "lengths": lengths, "input_norm_gain": input_norm_gain, "gate_matrix": gate_matrix, "input_matrix": input_matrix, "write_matrix": write_matrix, "read_matrix": read_matrix, "step_matrix": step_matrix, "step_size_bias": step_size_bias, "log_decay_rate": log_decay_rate, "direct_path_gain": direct_path_gain, "input_filter_taps": input_filter_taps, "write_filter_taps": write_filter_taps, "read_filter_taps": read_filter_taps, "position_log_decay": position_log_decay, "grouped_norm_gain": grouped_norm_gain, "output_matrix": output_matrix, "recurrent_head_state": recurrent_head_state, "history_input_rows": history_input_rows, "history_write_rows": history_write_rows, "history_read_rows": history_read_rows}


epsilon = 1e-06

def convolve(buffer, new_row, weights, tap_valid):
    tap_rows = weights.astype(jnp.float32)
    summed = new_row.astype(jnp.float32) * tap_rows[TAPS - 1]
    for k in range(TAPS - 1):
        summed = summed + buffer[:, k].astype(jnp.float32) * tap_rows[k] * tap_valid[:, k:k + 1]
    shifted = jnp.concatenate([buffer[:, 1:], new_row[:, None]], axis=1)
    return (jax.nn.silu(summed), shifted)

def per_sequence(seq_items):
    state_row, decay_row, step_row, value_heads, write_heads, read_heads = seq_items
    updated = decay_row[:, None, None] * state_row + (step_row[:, None] * value_heads)[:, :, None] * write_heads[:, None, :]
    readout = jnp.einsum('hpn,hn->hp', updated, read_heads, precision=lax.Precision.HIGHEST)
    return (updated, readout)

def reference(hidden, lengths, input_norm_gain, gate_matrix, input_matrix, write_matrix, read_matrix, step_matrix, step_size_bias, log_decay_rate, direct_path_gain, input_filter_taps, write_filter_taps, read_filter_taps, position_log_decay, grouped_norm_gain, output_matrix, recurrent_head_state, history_input_rows, history_write_rows, history_read_rows):
    per_group = MIXER_HEADS // GROUPS
    token_position = lengths - 1
    tap_valid = (jnp.arange(TAPS - 1)[None, :] >= TAPS - 1 - token_position[:, None]).astype(jnp.float32)
    state_is_valid = (token_position > 0).astype(jnp.float32)[:, None]
    position_indicator = (token_position[:, None] == jnp.arange(LONGEST_LENGTH)[None, :]).astype(jnp.float32)
    stream = hidden
    states, values, writes, reads = ([], [], [], [])
    for layer_index in range(MIXER_LAYERS):
        stream_float = stream.astype(jnp.float32)
        row_scale = lax.rsqrt(lax.optimization_barrier(jnp.mean(stream_float * stream_float, axis=1)) + epsilon)[:, None]
        normed = (stream_float * input_norm_gain[layer_index]).astype(jnp.bfloat16)
        proj_gate = jnp.dot(normed, gate_matrix[layer_index], preferred_element_type=jnp.float32) * row_scale
        proj_value = jnp.dot(normed, input_matrix[layer_index], preferred_element_type=jnp.float32) * row_scale
        proj_write = jnp.dot(normed, write_matrix[layer_index], preferred_element_type=jnp.float32) * row_scale
        proj_read = jnp.dot(normed, read_matrix[layer_index], preferred_element_type=jnp.float32) * row_scale
        proj_step = jnp.dot(normed, step_matrix[layer_index], preferred_element_type=jnp.float32) * row_scale
        value_act, value_buf = convolve(history_input_rows[layer_index], proj_value.astype(jnp.bfloat16), input_filter_taps[layer_index], tap_valid)
        write_act, write_buf = convolve(history_write_rows[layer_index], proj_write.astype(jnp.bfloat16), write_filter_taps[layer_index], tap_valid)
        read_act, read_buf = convolve(history_read_rows[layer_index], proj_read.astype(jnp.bfloat16), read_filter_taps[layer_index], tap_valid)
        head_step_size = jax.nn.softplus(proj_step + step_size_bias[layer_index])
        current_log_decay = jnp.dot(position_indicator, position_log_decay[layer_index], precision=lax.Precision.HIGHEST)
        current_decay = jnp.exp(-jnp.exp(log_decay_rate[layer_index]) * head_step_size + current_log_decay) * state_is_valid
        value_heads = value_act.reshape(SEQS, MIXER_HEADS, HEAD_DIM)
        write_heads = jnp.repeat(write_act.reshape(SEQS, GROUPS, STATE), per_group, axis=1)
        read_heads = jnp.repeat(read_act.reshape(SEQS, GROUPS, STATE), per_group, axis=1)
        updated, readout = lax.map(per_sequence, (recurrent_head_state[layer_index], current_decay, head_step_size, value_heads, write_heads, read_heads))
        mixed_heads = (readout + direct_path_gain[layer_index][None, :, None] * value_heads) * jax.nn.silu(proj_gate.reshape(SEQS, MIXER_HEADS, HEAD_DIM))
        grouped = mixed_heads.reshape(SEQS, GROUPS, per_group * HEAD_DIM)
        grouped = grouped * lax.rsqrt(lax.optimization_barrier(jnp.mean(grouped * grouped, axis=2, keepdims=True)) + epsilon)
        gated_rows = (grouped.reshape(SEQS, INNER) * grouped_norm_gain[layer_index]).astype(jnp.bfloat16)
        branch = jnp.dot(gated_rows, output_matrix[layer_index], preferred_element_type=jnp.float32)
        stream = (stream_float + branch).astype(jnp.bfloat16)
        states.append(updated)
        values.append(value_buf)
        writes.append(write_buf)
        reads.append(read_buf)
    return (stream, jnp.stack(states), jnp.stack(values), jnp.stack(writes), jnp.stack(reads))
```

```python
import functools

import jax
import jax.numpy as jnp
from jax import lax
from jax.experimental import pallas as pl
from jax.experimental.pallas import tpu as pltpu
from jax.sharding import PartitionSpec as P

MESH = pl.DeviceIdType.MESH
F32 = jnp.float32
BF16 = jnp.bfloat16
epsilon = 1e-06
LANES = 128
BLOCKS = 8
HIGH = lax.Precision.HIGHEST
LAST = (((1,), (1,)), ((), ()))


def far_first(count):
    return sorted(range(1, count), key=lambda o: -min(o, count - o))


def silu(z):
    return z / (1.0 + jnp.exp(-z))


def high_part(v):
    return v.astype(BF16).astype(F32)


def wait_bytes(ref, sem):
    pltpu.make_async_copy(ref, ref, sem).wait()


def lane_rows(block, first):
    return jnp.concatenate([block[first : first + 1], block[first + 1 : first + 2]], axis=1)


def kernel(
    n_dp,
    n_tp,
    hidden,
    lengths,
    in_gain,
    w_gate,
    w_value,
    w_write,
    w_read,
    w_step,
    step_bias,
    log_rate,
    direct_gain,
    taps_value,
    taps_write,
    taps_read,
    log_decay,
    group_gain,
    w_out,
    state_in,
    hist_value,
    hist_write,
    hist_read,
    stream_out,
    state_out,
    buf_value,
    buf_write,
    buf_read,
    part,
    rs_send,
    rs_recv,
    ag_send,
    ag_recv,
    gathered,
    ar_send,
    ar_recv,
    state,
    state_new,
    state_hi,
    state_lo,
    w_pack,
    conv_base,
    conv_last,
    tap_rows,
    decay_pad,
    head_pad,
    rs_ssem,
    rs_rsem,
    ag_ssem,
    ag_rsem,
    ar_ssem,
    ar_rsem,
    state_isem,
    state_osem,
):
    dp, tp = lax.axis_index("dp"), lax.axis_index("tp")
    layers, feats = in_gain.shape
    seqs = hidden.shape[0]
    width = feats * n_dp
    heads = step_bias.shape[1]
    inner = w_gate.shape[2]
    head_dim = inner // heads
    depth = hist_value.shape[1]
    half = seqs // 2

    barrier = pltpu.get_barrier_semaphore()
    for o in far_first(n_dp):
        pl.semaphore_signal(barrier, inc=1, device_id={"dp": lax.rem(dp + o, n_dp)}, device_id_type=MESH)
    for o in far_first(n_tp):
        pl.semaphore_signal(barrier, inc=1, device_id={"tp": lax.rem(tp + o, n_tp)}, device_id_type=MESH)
    loads = [pltpu.make_async_copy(state_in.at[l], state.at[l], state_isem.at[l]) for l in range(layers)]
    for c in loads:
        c.start()

    lane_seq = lax.broadcasted_iota(jnp.int32, (seqs, LANES), 1)
    lane_inner = lax.broadcasted_iota(jnp.int32, (2, inner), 1)
    pick = (
        lax.broadcasted_iota(jnp.int32, (w_step.shape[2], LANES), 0)
        == lax.broadcasted_iota(jnp.int32, (w_step.shape[2], LANES), 1) + tp * heads
    ) & (lax.broadcasted_iota(jnp.int32, (w_step.shape[2], LANES), 1) < heads)
    pick = pick.astype(F32).astype(BF16)

    def per_head(rows):
        out = jnp.broadcast_to(rows[:, heads - 1 : heads], (rows.shape[0], inner))
        lane = lane_inner[: rows.shape[0]]
        for h in range(heads - 2, -1, -1):
            out = jnp.where(lane < (h + 1) * head_dim, rows[:, h : h + 1], out)
        return out

    def project(l, x):
        normed = (x * in_gain[l : l + 1, :]).astype(BF16)
        columns = []
        for w in (w_gate, w_value, w_write, w_read):
            r = jnp.dot(normed, w[l], preferred_element_type=F32)
            for at in range(0, r.shape[1], LANES):
                columns.append(r[:, at : at + LANES])
        w_mine = jnp.dot(w_step[l], pick, preferred_element_type=F32).astype(BF16)
        step = jnp.dot(normed, w_mine, preferred_element_type=F32)
        square = jnp.sum(x * x, axis=1, keepdims=True)
        rest = jnp.where(lane_seq == heads, square, step)
        high = high_part(rest)
        columns += [high, rest - high]
        for c, column in enumerate(columns):
            part[pl.ds(c, seqs, stride=BLOCKS), :] = column
        rs_send[l] = part[...].reshape(n_dp, 2 * BLOCKS, LANES).astype(BF16)

    def send_partials(l):
        for o in far_first(n_dp):
            to = lax.rem(dp + o, n_dp)
            pltpu.make_async_remote_copy(
                src_ref=rs_send.at[l, to],
                dst_ref=rs_recv.at[l, dp],
                send_sem=rs_ssem.at[l],
                recv_sem=rs_rsem.at[l],
                device_id={"dp": to},
                device_id_type=MESH,
            ).start()
        rs_recv[l, dp] = rs_send[l, dp]

    def send_gated(l):
        for o in far_first(n_dp):
            pltpu.make_async_remote_copy(
                src_ref=ag_send.at[l],
                dst_ref=ag_recv.at[l, dp],
                send_sem=ag_ssem.at[l],
                recv_sem=ag_rsem.at[l],
                device_id={"dp": lax.rem(dp + o, n_dp)},
                device_id_type=MESH,
            ).start()
        ag_recv[l, dp] = ag_send[l]

    def send_branch(l):
        for o in far_first(n_tp):
            pltpu.make_async_remote_copy(
                src_ref=ar_send.at[l],
                dst_ref=ar_recv.at[l, tp],
                send_sem=ar_ssem.at[l],
                recv_sem=ar_rsem.at[l],
                device_id={"tp": lax.rem(tp + o, n_tp)},
                device_id_type=MESH,
            ).start()
        ar_recv[l, tp] = ar_send[l]

    x_bf = hidden[...]
    project(0, x_bf.astype(F32))

    position = [lengths[s] - 1 for s in range(2)]
    row8 = lax.broadcasted_iota(jnp.int32, (8, log_decay.shape[2]), 0)
    lane_pos = lax.broadcasted_iota(jnp.int32, (8, log_decay.shape[2]), 1)
    at_position = (lane_pos == jnp.where(row8 == 0, position[0], position[1])).astype(F32)
    row2 = lax.broadcasted_iota(jnp.int32, (2, LANES), 0)
    is_live = jnp.where(jnp.where(row2 == 0, position[0], position[1]) > 0, 1.0, 0.0)
    conv_base[...] = jnp.zeros_like(conv_base)
    conv_last[...] = jnp.zeros_like(conv_last)
    decay_pad[...] = jnp.zeros_like(decay_pad)
    head_pad[...] = jnp.zeros_like(head_pad)
    w_pack[...] = jnp.zeros_like(w_pack)
    decay_log = []
    for l in range(layers):
        decay_pad[l, 0:heads, :] = log_decay[l]
        picked = lax.dot_general(at_position, decay_pad[l], LAST, precision=HIGH, preferred_element_type=F32)
        decay_log.append(picked[0:2])
        head_pad[l, 0:1, 0:heads] = step_bias[l : l + 1, :]
        head_pad[l, 1:2, 0:heads] = jnp.exp(log_rate[l : l + 1, :])
        w_pack[l, 0:feats, 0:inner] = w_out[l]
        w_pack[l, feats : 2 * feats, inner : 2 * inner] = w_out[l]
        for taps, hist, row in (
            (taps_value, hist_value, 2),
            (taps_write, hist_write, 4),
            (taps_read, hist_read, 5),
        ):
            tap = taps[l].astype(F32)
            total = None
            for k in range(depth):
                rows = hist[l, k].astype(F32)
                valid = jnp.where(
                    lax.broadcasted_iota(jnp.int32, rows.shape, 0) == 0,
                    jnp.where(k >= depth - position[0], 1.0, 0.0),
                    jnp.where(k >= depth - position[1], 1.0, 0.0),
                )
                term = rows * tap[k : k + 1] * valid
                total = term if total is None else total + term
            for c in range(rows.shape[1] // LANES):
                for s in range(2):
                    at = s * BLOCKS + row + c
                    conv_base[l, at : at + 1, :] = total[s : s + 1, c * LANES : (c + 1) * LANES]
                    conv_last[l, at : at + 1, :] = tap[depth : depth + 1, c * LANES : (c + 1) * LANES]
    for l in range(layers):
        loads[l].wait()
        high = state[l].astype(BF16)
        state_hi[l] = high
        state_lo[l] = (state[l] - high.astype(F32)).astype(BF16)

    pl.semaphore_wait(barrier, n_dp - 1 + n_tp - 1)

    row16 = lax.broadcasted_iota(jnp.int32, (2 * BLOCKS, LANES), 0)
    is_gate = lax.rem(row16, BLOCKS) < 2
    row_of8 = lax.broadcasted_iota(jnp.int32, (8, LANES), 0)
    stores = []
    x_pack = jnp.concatenate([x_bf[:half].astype(F32), x_bf[half:].astype(F32)], axis=1)
    for l in range(layers):
        send_partials(l)
        wait_bytes(rs_recv.at[l, pl.ds(0, n_dp - 1)], rs_rsem.at[l])
        summed = jnp.sum(rs_recv[l].astype(F32), axis=0)
        rest = jnp.concatenate(
            [summed[BLOCKS * s + 6 : BLOCKS * s + 7] + summed[BLOCKS * s + 7 : BLOCKS * s + 8] for s in range(2)], axis=0
        )
        row_scale = lax.rsqrt(rest[:, heads : heads + 1] / width + epsilon)
        scale16 = jnp.where(row16 < BLOCKS, row_scale[0:1], row_scale[1:2])
        scaled = summed * scale16
        current = high_part(scaled)
        act = silu(jnp.where(is_gate, scaled, conv_base[l] + current * conv_last[l]))
        z = rest * row_scale + head_pad[l, 0:1, :]
        step = jnp.maximum(z, 0.0) + jnp.log1p(jnp.exp(-jnp.abs(z)))
        decay = jnp.exp(decay_log[l] - head_pad[l, 1:2, :] * step) * is_live
        gate_row = jnp.concatenate([lane_rows(act, BLOCKS * s) for s in range(2)], axis=0)
        value_row = jnp.concatenate([lane_rows(act, BLOCKS * s + 2) for s in range(2)], axis=0)
        step_value = per_head(step) * value_row
        decay_row = per_head(decay)
        readout, along = [], []
        for s in range(2):
            write = act[BLOCKS * s + 4 : BLOCKS * s + 5]
            read = act[BLOCKS * s + 5 : BLOCKS * s + 6]
            high = high_part(read)
            lhs = jnp.where(row_of8 == 0, high, jnp.where(row_of8 == 1, read - high, 0.0)).astype(BF16)
            a = lax.dot_general(lhs, state_hi[l, s], LAST, preferred_element_type=F32)
            b = lax.dot_general(lhs, state_lo[l, s], LAST, preferred_element_type=F32)
            readout.append(a[0:1] + a[1:2] + b[0:1])
            along.append(jnp.sum(write * read, axis=1, keepdims=True))
        readout = jnp.concatenate(readout, axis=0)
        along = jnp.concatenate(along, axis=0)
        mixed = (
            decay_row * readout + step_value * along + per_head(direct_gain[l : l + 1, :]) * value_row
        ) * gate_row
        mean = jnp.sum(mixed * mixed, axis=1, keepdims=True) / inner
        gated = mixed * lax.rsqrt(mean + epsilon) * group_gain[l : l + 1, :]
        ag_send[l] = gated.astype(BF16)
        send_gated(l)

        for b in range(inner // LANES):
            cols = jnp.transpose(
                jnp.concatenate(
                    [step_value[:, b * LANES : (b + 1) * LANES], jnp.zeros((6, LANES), F32)], axis=0
                )
            )
            for s in range(2):
                write = act[BLOCKS * s + 4 : BLOCKS * s + 5]
                for j in range(LANES // head_dim):
                    h = b * (LANES // head_dim) + j
                    at = slice(h * head_dim, (h + 1) * head_dim)
                    state_new[l, s, at, :] = (
                        decay[s : s + 1, h : h + 1] * state[l, s, at, :]
                        + cols[j * head_dim : (j + 1) * head_dim, s : s + 1] * write
                    )
        stores.append(pltpu.make_async_copy(state_new.at[l], state_out.at[l], state_osem.at[l]))
        stores[-1].start()
        for k in range(depth - 1):
            buf_value[l, k] = hist_value[l, k + 1]
            buf_write[l, k] = hist_write[l, k + 1]
            buf_read[l, k] = hist_read[l, k + 1]
        buf_value[l, depth - 1] = jnp.concatenate(
            [lane_rows(current, BLOCKS * s + 2) for s in range(2)], axis=0
        ).astype(BF16)
        buf_write[l, depth - 1] = jnp.concatenate(
            [current[BLOCKS * s + 4 : BLOCKS * s + 5] for s in range(2)], axis=0
        ).astype(BF16)
        buf_read[l, depth - 1] = jnp.concatenate(
            [current[BLOCKS * s + 5 : BLOCKS * s + 6] for s in range(2)], axis=0
        ).astype(BF16)

        wait_bytes(ag_recv.at[l, pl.ds(0, n_dp - 1)], ag_rsem.at[l])
        for d in range(n_dp):
            gathered[2 * d : 2 * d + 2, :] = ag_recv[l, d].astype(F32)
        rows = jnp.concatenate([gathered[0:half, :], gathered[half:, :]], axis=1).astype(BF16)
        branch = lax.dot_general(rows, w_pack[l], LAST, preferred_element_type=F32)
        ar_send[l] = branch.astype(BF16)
        send_branch(l)
        wait_bytes(ar_recv.at[l, pl.ds(0, n_tp - 1)], ar_rsem.at[l])
        x_pack = high_part(x_pack + jnp.sum(ar_recv[l].astype(F32), axis=0))
        x = jnp.concatenate([x_pack[:, :feats], x_pack[:, feats:]], axis=0)
        if l + 1 < layers:
            project(l + 1, x)
    stream_out[...] = x.astype(BF16)
    for l in range(layers):
        wait_bytes(rs_send.at[l, pl.ds(0, n_dp - 1)], rs_ssem.at[l])
        wait_bytes(ag_recv.at[l, pl.ds(0, n_dp - 1)], ag_ssem.at[l])
        wait_bytes(ar_recv.at[l, pl.ds(0, n_tp - 1)], ar_ssem.at[l])
        stores[l].wait()


def on_device(
    hidden,
    lengths,
    input_norm_gain,
    gate_matrix,
    input_matrix,
    write_matrix,
    read_matrix,
    step_matrix,
    step_size_bias,
    log_decay_rate,
    direct_path_gain,
    input_filter_taps,
    write_filter_taps,
    read_filter_taps,
    position_log_decay,
    grouped_norm_gain,
    output_matrix,
    recurrent_head_state,
    history_input_rows,
    history_write_rows,
    history_read_rows,
):
    n_dp, n_tp = lax.axis_size("dp"), lax.axis_size("tp")
    layers, seq_local, heads, head_dim, state_dim = recurrent_head_state.shape
    inner = heads * head_dim
    seqs, feats = hidden.shape
    assert seq_local == 2 and state_dim == LANES and write_matrix.shape[2] == LANES and inner == 2 * LANES
    state_shape = (layers, seq_local, inner, state_dim)
    operands = (
        hidden,
        lengths,
        input_norm_gain,
        gate_matrix,
        input_matrix,
        write_matrix,
        read_matrix,
        step_matrix,
        step_size_bias,
        log_decay_rate,
        direct_path_gain,
        input_filter_taps,
        write_filter_taps,
        read_filter_taps,
        position_log_decay.transpose(0, 2, 1),
        grouped_norm_gain,
        output_matrix.transpose(0, 2, 1),
        recurrent_head_state.reshape(state_shape),
        history_input_rows.transpose(0, 2, 1, 3),
        history_write_rows.transpose(0, 2, 1, 3),
        history_read_rows.transpose(0, 2, 1, 3),
    )
    vmem, anywhere = pl.BlockSpec(memory_space=pltpu.VMEM), pl.BlockSpec(memory_space=pl.ANY)
    in_specs = [vmem] * len(operands)
    in_specs[1] = pl.BlockSpec(memory_space=pltpu.SMEM)
    in_specs[17] = anywhere
    taken = lambda a: jax.ShapeDtypeStruct(a.shape, a.dtype)
    positions = position_log_decay.shape[1]
    dma = pltpu.SemaphoreType.DMA
    stream, states, values, writes, reads = pl.pallas_call(
        functools.partial(kernel, n_dp, n_tp),
        out_shape=(
            taken(hidden),
            taken(operands[17]),
            taken(operands[18]),
            taken(operands[19]),
            taken(operands[20]),
        ),
        in_specs=in_specs,
        out_specs=(vmem, anywhere, vmem, vmem, vmem),
        scratch_shapes=[
            pltpu.VMEM((seqs * BLOCKS, LANES), F32),
            pltpu.VMEM((layers, n_dp, 2 * BLOCKS, LANES), BF16),
            pltpu.VMEM((layers, n_dp, 2 * BLOCKS, LANES), BF16),
            pltpu.VMEM((layers, 2, inner), BF16),
            pltpu.VMEM((layers, n_dp, 2, inner), BF16),
            pltpu.VMEM((seqs, inner), F32),
            pltpu.VMEM((layers, seqs // 2, 2 * feats), BF16),
            pltpu.VMEM((layers, n_tp, seqs // 2, 2 * feats), BF16),
            pltpu.VMEM(state_shape, F32),
            pltpu.VMEM(state_shape, F32),
            pltpu.VMEM(state_shape, BF16),
            pltpu.VMEM(state_shape, BF16),
            pltpu.VMEM((layers, 2 * feats, 2 * inner), BF16),
            pltpu.VMEM((layers, 2 * BLOCKS, LANES), F32),
            pltpu.VMEM((layers, 2 * BLOCKS, LANES), F32),
            pltpu.VMEM((8, LANES), F32),
            pltpu.VMEM((layers, LANES, positions), F32),
            pltpu.VMEM((layers, 8, LANES), F32),
        ]
        + [dma((layers,))] * 8,
        compiler_params=pltpu.CompilerParams(collective_id=0, has_side_effects=True),
        name="mixers",
    )(*operands)
    return (
        stream,
        states.reshape(recurrent_head_state.shape),
        values.transpose(0, 2, 1, 3),
        writes.transpose(0, 2, 1, 3),
        reads.transpose(0, 2, 1, 3),
    )


def solution(mesh):
    placed = (
        P("grp", "dp"),
        P(("grp", "dp")),
        P(None, "dp"),
        P(None, "dp", "tp"),
        P(None, "dp", "tp"),
        P(None, "dp", "tp"),
        P(None, "dp", "tp"),
        P(None, "dp", None),
        P(None, "tp"),
        P(None, "tp"),
        P(None, "tp"),
        P(None, None, "tp"),
        P(None, None, "tp"),
        P(None, None, "tp"),
        P(None, None, "tp"),
        P(None, "tp"),
        P(None, "tp", "dp"),
        P(None, ("grp", "dp"), "tp", None, None),
        P(None, ("grp", "dp"), None, "tp"),
        P(None, ("grp", "dp"), None, "tp"),
        P(None, ("grp", "dp"), None, "tp"),
    )
    return jax.shard_map(
        on_device,
        mesh=mesh,
        in_specs=placed,
        out_specs=(
            P("grp", "dp"),
            P(None, ("grp", "dp"), "tp", None, None),
            P(None, ("grp", "dp"), None, "tp"),
            P(None, ("grp", "dp"), None, "tp"),
            P(None, ("grp", "dp"), None, "tp"),
        ),
        check_vma=False,
    )
```

```python
import functools

import jax
import jax.numpy as jnp
from jax import lax
from jax.experimental import pallas as pl
from jax.experimental.pallas import tpu as pltpu
from jax.sharding import PartitionSpec as P

MESH = pl.DeviceIdType.MESH
F32 = jnp.float32
BF16 = jnp.bfloat16
epsilon = 1e-06
LANES = 128
BLOCKS = 8
HIGH = lax.Precision.HIGHEST
LAST = (((1,), (1,)), ((), ()))


def far_first(count):
    return sorted(range(1, count), key=lambda o: -min(o, count - o))


def silu(z):
    return z / (1.0 + jnp.exp(-z))


def high_part(v):
    return v.astype(BF16).astype(F32)


def wait_bytes(ref, sem):
    pltpu.make_async_copy(ref, ref, sem).wait()


def lane_rows(block, first):
    return jnp.concatenate([block[first : first + 1], block[first + 1 : first + 2]], axis=1)


def flush(*refs):
    count = len(refs) // 2
    sems = refs[-1]
    copies = [pltpu.make_async_copy(refs[i], refs[count + i], sems.at[i]) for i in range(count)]
    for c in copies:
        c.start()
    for c in copies:
        c.wait()


def kernel(n_dp, n_tp, *refs):
    given, rest = refs[:21], refs[21:]
    outs, held, rest = rest[:5], rest[5:24], rest[24:]
    scratch, in_sem = rest[:-1], rest[-1]
    lengths, state_in = given[1], given[17]
    whole = [g for i, g in enumerate(given) if i not in (1, 17)]
    barrier = pltpu.get_barrier_semaphore()
    dp, tp = lax.axis_index("dp"), lax.axis_index("tp")
    state = scratch[9]
    loads = [pltpu.make_async_copy(g, h, in_sem.at[i]) for i, (g, h) in enumerate(zip(whole, held))]
    loads.append(pltpu.make_async_copy(state_in, state, in_sem.at[len(whole)]))
    for c in loads[:8]:
        c.start()
    for o in far_first(n_dp):
        pl.semaphore_signal(barrier, inc=1, device_id={"dp": lax.rem(dp + o, n_dp)}, device_id_type=MESH)
    for c in loads[8:]:
        c.start()
    for o in far_first(n_tp):
        pl.semaphore_signal(barrier, inc=1, device_id={"tp": lax.rem(tp + o, n_tp)}, device_id_type=MESH)
    held = list(held)
    held.insert(1, lengths)
    body(n_dp, n_tp, barrier, loads, *held, *outs, *scratch)


def body(
    n_dp,
    n_tp,
    barrier,
    loads,
    hidden,
    lengths,
    in_gain,
    w_gate,
    w_value,
    w_write,
    w_read,
    w_step,
    step_bias,
    log_rate,
    direct_gain,
    taps_value,
    taps_write,
    taps_read,
    log_decay,
    group_gain,
    w_out,
    hist_value,
    hist_write,
    hist_read,
    stream_out,
    state_new,
    buf_value,
    buf_write,
    buf_read,
    part,
    rs_send,
    rs_recv,
    ag_send,
    ag_recv,
    gathered,
    ar_send,
    ar_recv,
    spare,
    state,
    state_hi,
    state_lo,
    w_pack,
    conv_base,
    conv_last,
    decay_pad,
    head_pad,
    rs_ssem,
    rs_rsem,
    ag_ssem,
    ag_rsem,
    ar_ssem,
    ar_rsem,
):
    dp, tp = lax.axis_index("dp"), lax.axis_index("tp")
    layers, feats = in_gain.shape
    seqs = hidden.shape[0]
    width = feats * n_dp
    heads = step_bias.shape[1]
    inner = w_gate.shape[2]
    head_dim = inner // heads
    depth = hist_value.shape[1]
    half = seqs // 2

    lane_seq = lax.broadcasted_iota(jnp.int32, (seqs, LANES), 1)
    lane_inner = lax.broadcasted_iota(jnp.int32, (2, inner), 1)
    pick = (
        lax.broadcasted_iota(jnp.int32, (w_step.shape[2], LANES), 0)
        == lax.broadcasted_iota(jnp.int32, (w_step.shape[2], LANES), 1) + tp * heads
    ) & (lax.broadcasted_iota(jnp.int32, (w_step.shape[2], LANES), 1) < heads)
    pick = pick.astype(F32).astype(BF16)

    def per_head(rows):
        out = jnp.broadcast_to(rows[:, heads - 1 : heads], (rows.shape[0], inner))
        lane = lane_inner[: rows.shape[0]]
        for h in range(heads - 2, -1, -1):
            out = jnp.where(lane < (h + 1) * head_dim, rows[:, h : h + 1], out)
        return out

    def project(l, x):
        normed = (x * in_gain[l : l + 1, :]).astype(BF16)
        columns = []
        for w in (w_gate, w_value, w_write, w_read):
            r = jnp.dot(normed, w[l], preferred_element_type=F32)
            for at in range(0, r.shape[1], LANES):
                columns.append(r[:, at : at + LANES])
        w_mine = jnp.dot(w_step[l], pick, preferred_element_type=F32).astype(BF16)
        step = jnp.dot(normed, w_mine, preferred_element_type=F32)
        square = jnp.sum(x * x, axis=1, keepdims=True)
        rest = jnp.where(lane_seq == heads, square, step)
        high = high_part(rest)
        columns += [high, rest - high]
        for c, column in enumerate(columns):
            part[pl.ds(c, seqs, stride=BLOCKS), :] = column
        rs_send[l] = part[...].reshape(n_dp, 2 * BLOCKS, LANES).astype(BF16)

    def send_partials(l):
        for o in far_first(n_dp):
            to = lax.rem(dp + o, n_dp)
            pltpu.make_async_remote_copy(
                src_ref=rs_send.at[l, to],
                dst_ref=rs_recv.at[l, dp],
                send_sem=rs_ssem.at[l],
                recv_sem=rs_rsem.at[l],
                device_id={"dp": to},
                device_id_type=MESH,
            ).start()
        rs_recv[l, dp] = rs_send[l, dp]

    def send_gated(l):
        for o in far_first(n_dp):
            pltpu.make_async_remote_copy(
                src_ref=ag_send.at[l],
                dst_ref=ag_recv.at[l, dp],
                send_sem=ag_ssem.at[l],
                recv_sem=ag_rsem.at[l],
                device_id={"dp": lax.rem(dp + o, n_dp)},
                device_id_type=MESH,
            ).start()
        ag_recv[l, dp] = ag_send[l]

    def send_branch(l):
        for o in far_first(n_tp):
            pltpu.make_async_remote_copy(
                src_ref=ar_send.at[l],
                dst_ref=ar_recv.at[l, tp],
                send_sem=ar_ssem.at[l],
                recv_sem=ar_rsem.at[l],
                device_id={"tp": lax.rem(tp + o, n_tp)},
                device_id_type=MESH,
            ).start()
        ar_recv[l, tp] = ar_send[l]

    for c in loads[:7]:
        c.wait()
    x_bf = hidden[...]
    project(0, x_bf.astype(F32))

    for c in loads[7:]:
        c.wait()
    position = [lengths[s] - 1 for s in range(2)]
    row8 = lax.broadcasted_iota(jnp.int32, (8, log_decay.shape[2]), 0)
    lane_pos = lax.broadcasted_iota(jnp.int32, (8, log_decay.shape[2]), 1)
    at_position = (lane_pos == jnp.where(row8 == 0, position[0], position[1])).astype(F32)
    row2 = lax.broadcasted_iota(jnp.int32, (2, LANES), 0)
    is_live = jnp.where(jnp.where(row2 == 0, position[0], position[1]) > 0, 1.0, 0.0)
    conv_base[...] = jnp.zeros_like(conv_base)
    conv_last[...] = jnp.zeros_like(conv_last)
    decay_pad[...] = jnp.zeros_like(decay_pad)
    head_pad[...] = jnp.zeros_like(head_pad)
    w_pack[...] = jnp.zeros_like(w_pack)
    decay_log = []
    for l in range(layers):
        decay_pad[l, 0:heads, :] = log_decay[l]
        picked = lax.dot_general(at_position, decay_pad[l], LAST, precision=HIGH, preferred_element_type=F32)
        decay_log.append(picked[0:2])
        head_pad[l, 0:1, 0:heads] = step_bias[l : l + 1, :]
        head_pad[l, 1:2, 0:heads] = jnp.exp(log_rate[l : l + 1, :])
        w_pack[l, 0:feats, 0:inner] = w_out[l]
        w_pack[l, feats : 2 * feats, inner : 2 * inner] = w_out[l]
        for taps, hist, row in (
            (taps_value, hist_value, 2),
            (taps_write, hist_write, 4),
            (taps_read, hist_read, 5),
        ):
            tap = taps[l].astype(F32)
            total = None
            for k in range(depth):
                rows = hist[l, k].astype(F32)
                valid = jnp.where(
                    lax.broadcasted_iota(jnp.int32, rows.shape, 0) == 0,
                    jnp.where(k >= depth - position[0], 1.0, 0.0),
                    jnp.where(k >= depth - position[1], 1.0, 0.0),
                )
                term = rows * tap[k : k + 1] * valid
                total = term if total is None else total + term
            for c in range(rows.shape[1] // LANES):
                for s in range(2):
                    at = s * BLOCKS + row + c
                    conv_base[l, at : at + 1, :] = total[s : s + 1, c * LANES : (c + 1) * LANES]
                    conv_last[l, at : at + 1, :] = tap[depth : depth + 1, c * LANES : (c + 1) * LANES]
    for l in range(layers):
        high = state[l].astype(BF16)
        state_hi[l] = high
        state_lo[l] = (state[l] - high.astype(F32)).astype(BF16)

    pl.semaphore_wait(barrier, n_dp - 1 + n_tp - 1)

    row16 = lax.broadcasted_iota(jnp.int32, (2 * BLOCKS, LANES), 0)
    is_gate = lax.rem(row16, BLOCKS) < 2
    row_of8 = lax.broadcasted_iota(jnp.int32, (8, LANES), 0)
    x_pack = jnp.concatenate([x_bf[:half].astype(F32), x_bf[half:].astype(F32)], axis=1)
    for l in range(layers):
        send_partials(l)
        wait_bytes(rs_recv.at[l, pl.ds(0, n_dp - 1)], rs_rsem.at[l])
        summed = jnp.sum(rs_recv[l].astype(F32), axis=0)
        rest = jnp.concatenate(
            [summed[BLOCKS * s + 6 : BLOCKS * s + 7] + summed[BLOCKS * s + 7 : BLOCKS * s + 8] for s in range(2)], axis=0
        )
        row_scale = lax.rsqrt(rest[:, heads : heads + 1] / width + epsilon)
        scale16 = jnp.where(row16 < BLOCKS, row_scale[0:1], row_scale[1:2])
        scaled = summed * scale16
        current = high_part(scaled)
        act = silu(jnp.where(is_gate, scaled, conv_base[l] + current * conv_last[l]))
        z = rest * row_scale + head_pad[l, 0:1, :]
        step = jnp.maximum(z, 0.0) + jnp.log1p(jnp.exp(-jnp.abs(z)))
        decay = jnp.exp(decay_log[l] - head_pad[l, 1:2, :] * step) * is_live
        gate_row = jnp.concatenate([lane_rows(act, BLOCKS * s) for s in range(2)], axis=0)
        value_row = jnp.concatenate([lane_rows(act, BLOCKS * s + 2) for s in range(2)], axis=0)
        step_value = per_head(step) * value_row
        decay_row = per_head(decay)
        readout, along = [], []
        for s in range(2):
            write = act[BLOCKS * s + 4 : BLOCKS * s + 5]
            read = act[BLOCKS * s + 5 : BLOCKS * s + 6]
            high = high_part(read)
            lhs = jnp.where(row_of8 == 0, high, jnp.where(row_of8 == 1, read - high, 0.0)).astype(BF16)
            a = lax.dot_general(lhs, state_hi[l, s], LAST, preferred_element_type=F32)
            b = lax.dot_general(lhs, state_lo[l, s], LAST, preferred_element_type=F32)
            readout.append(a[0:1] + a[1:2] + b[0:1])
            along.append(jnp.sum(write * read, axis=1, keepdims=True))
        readout = jnp.concatenate(readout, axis=0)
        along = jnp.concatenate(along, axis=0)
        mixed = (
            decay_row * readout + step_value * along + per_head(direct_gain[l : l + 1, :]) * value_row
        ) * gate_row
        mean = jnp.sum(mixed * mixed, axis=1, keepdims=True) / inner
        gated = mixed * lax.rsqrt(mean + epsilon) * group_gain[l : l + 1, :]
        ag_send[l] = gated.astype(BF16)
        send_gated(l)

        for b in range(inner // LANES):
            cols = jnp.transpose(
                jnp.concatenate(
                    [step_value[:, b * LANES : (b + 1) * LANES], jnp.zeros((6, LANES), F32)], axis=0
                )
            )
            for s in range(2):
                write = act[BLOCKS * s + 4 : BLOCKS * s + 5]
                for j in range(LANES // head_dim):
                    h = b * (LANES // head_dim) + j
                    at = slice(h * head_dim, (h + 1) * head_dim)
                    state_new[l, s, at, :] = (
                        decay[s : s + 1, h : h + 1] * state[l, s, at, :]
                        + cols[j * head_dim : (j + 1) * head_dim, s : s + 1] * write
                    )
        for k in range(depth - 1):
            buf_value[l, k] = hist_value[l, k + 1]
            buf_write[l, k] = hist_write[l, k + 1]
            buf_read[l, k] = hist_read[l, k + 1]
        buf_value[l, depth - 1] = jnp.concatenate(
            [lane_rows(current, BLOCKS * s + 2) for s in range(2)], axis=0
        ).astype(BF16)
        buf_write[l, depth - 1] = jnp.concatenate(
            [current[BLOCKS * s + 4 : BLOCKS * s + 5] for s in range(2)], axis=0
        ).astype(BF16)
        buf_read[l, depth - 1] = jnp.concatenate(
            [current[BLOCKS * s + 5 : BLOCKS * s + 6] for s in range(2)], axis=0
        ).astype(BF16)

        wait_bytes(ag_recv.at[l, pl.ds(0, n_dp - 1)], ag_rsem.at[l])
        for d in range(n_dp):
            gathered[2 * d : 2 * d + 2, :] = ag_recv[l, d].astype(F32)
        rows = jnp.concatenate([gathered[0:half, :], gathered[half:, :]], axis=1).astype(BF16)
        branch = lax.dot_general(rows, w_pack[l], LAST, preferred_element_type=F32)
        ar_send[l] = branch.astype(BF16)
        send_branch(l)
        wait_bytes(ar_recv.at[l, pl.ds(0, n_tp - 1)], ar_rsem.at[l])
        x_pack = high_part(x_pack + jnp.sum(ar_recv[l].astype(F32), axis=0))
        x = jnp.concatenate([x_pack[:, :feats], x_pack[:, feats:]], axis=0)
        if l + 1 < layers:
            project(l + 1, x)
    stream_out[...] = x.astype(BF16)
    for l in range(layers):
        wait_bytes(rs_send.at[l, pl.ds(0, n_dp - 1)], rs_ssem.at[l])
        wait_bytes(ag_recv.at[l, pl.ds(0, n_dp - 1)], ag_ssem.at[l])
        wait_bytes(ar_recv.at[l, pl.ds(0, n_tp - 1)], ar_ssem.at[l])


def on_device(
    hidden,
    lengths,
    input_norm_gain,
    gate_matrix,
    input_matrix,
    write_matrix,
    read_matrix,
    step_matrix,
    step_size_bias,
    log_decay_rate,
    direct_path_gain,
    input_filter_taps,
    write_filter_taps,
    read_filter_taps,
    position_log_decay,
    grouped_norm_gain,
    output_matrix,
    recurrent_head_state,
    history_input_rows,
    history_write_rows,
    history_read_rows,
):
    n_dp, n_tp = lax.axis_size("dp"), lax.axis_size("tp")
    layers, seq_local, heads, head_dim, state_dim = recurrent_head_state.shape
    inner = heads * head_dim
    seqs, feats = hidden.shape
    assert seq_local == 2 and state_dim == LANES and write_matrix.shape[2] == LANES and inner == 2 * LANES
    state_shape = (layers, seq_local, inner, state_dim)
    operands = (
        hidden,
        lengths,
        input_norm_gain,
        gate_matrix,
        input_matrix,
        write_matrix,
        read_matrix,
        step_matrix,
        step_size_bias,
        log_decay_rate,
        direct_path_gain,
        input_filter_taps,
        write_filter_taps,
        read_filter_taps,
        position_log_decay.transpose(0, 2, 1),
        grouped_norm_gain,
        output_matrix.transpose(0, 2, 1),
        recurrent_head_state.reshape(state_shape),
        history_input_rows.transpose(0, 2, 1, 3),
        history_write_rows.transpose(0, 2, 1, 3),
        history_read_rows.transpose(0, 2, 1, 3),
    )
    vmem, hbm = pl.BlockSpec(memory_space=pltpu.VMEM), pl.BlockSpec(memory_space=pltpu.HBM)
    in_specs = [hbm] * len(operands)
    in_specs[1] = pl.BlockSpec(memory_space=pltpu.SMEM)
    results = [operands[i] for i in (0, 17, 18, 19, 20)]
    positions = position_log_decay.shape[1]
    dma = pltpu.SemaphoreType.DMA
    whole = [o for i, o in enumerate(operands) if i not in (1, 17)]
    finished = pl.pallas_call(
        functools.partial(kernel, n_dp, n_tp),
        out_shape=[pltpu.VMEM(r.shape, r.dtype) for r in results],
        in_specs=in_specs,
        out_specs=[vmem] * len(results),
        scratch_shapes=[pltpu.VMEM(o.shape, o.dtype) for o in whole]
        + [
            pltpu.VMEM((seqs * BLOCKS, LANES), F32),
            pltpu.VMEM((layers, n_dp, 2 * BLOCKS, LANES), BF16),
            pltpu.VMEM((layers, n_dp, 2 * BLOCKS, LANES), BF16),
            pltpu.VMEM((layers, 2, inner), BF16),
            pltpu.VMEM((layers, n_dp, 2, inner), BF16),
            pltpu.VMEM((seqs, inner), F32),
            pltpu.VMEM((layers, seqs // 2, 2 * feats), BF16),
            pltpu.VMEM((layers, n_tp, seqs // 2, 2 * feats), BF16),
            pltpu.VMEM((8, LANES), F32),
            pltpu.VMEM(state_shape, F32),
            pltpu.VMEM(state_shape, BF16),
            pltpu.VMEM(state_shape, BF16),
            pltpu.VMEM((layers, 2 * feats, 2 * inner), BF16),
            pltpu.VMEM((layers, 2 * BLOCKS, LANES), F32),
            pltpu.VMEM((layers, 2 * BLOCKS, LANES), F32),
            pltpu.VMEM((layers, LANES, positions), F32),
            pltpu.VMEM((layers, 8, LANES), F32),
        ]
        + [dma((layers,))] * 6
        + [dma((len(whole) + 1,))],
        compiler_params=pltpu.CompilerParams(
            collective_id=0, has_side_effects=True
        ),
        name="mixers",
    )(*operands)
    stream, states, values, writes, reads = pl.pallas_call(
        flush,
        out_shape=[jax.ShapeDtypeStruct(r.shape, r.dtype) for r in results],
        in_specs=[vmem] * len(results),
        out_specs=[hbm] * len(results),
        scratch_shapes=[dma((len(results),))],
        compiler_params=pltpu.CompilerParams(vmem_limit_bytes=4 * 1024 * 1024),
        name="flush",
    )(*finished)
    return (
        stream,
        states.reshape(recurrent_head_state.shape),
        values.transpose(0, 2, 1, 3),
        writes.transpose(0, 2, 1, 3),
        reads.transpose(0, 2, 1, 3),
    )


def solution(mesh):
    placed = (
        P("grp", "dp"),
        P(("grp", "dp")),
        P(None, "dp"),
        P(None, "dp", "tp"),
        P(None, "dp", "tp"),
        P(None, "dp", "tp"),
        P(None, "dp", "tp"),
        P(None, "dp", None),
        P(None, "tp"),
        P(None, "tp"),
        P(None, "tp"),
        P(None, None, "tp"),
        P(None, None, "tp"),
        P(None, None, "tp"),
        P(None, None, "tp"),
        P(None, "tp"),
        P(None, "tp", "dp"),
        P(None, ("grp", "dp"), "tp", None, None),
        P(None, ("grp", "dp"), None, "tp"),
        P(None, ("grp", "dp"), None, "tp"),
        P(None, ("grp", "dp"), None, "tp"),
    )
    return jax.shard_map(
        on_device,
        mesh=mesh,
        in_specs=placed,
        out_specs=(
            P("grp", "dp"),
            P(None, ("grp", "dp"), "tp", None, None),
            P(None, ("grp", "dp"), None, "tp"),
            P(None, ("grp", "dp"), None, "tp"),
            P(None, ("grp", "dp"), None, "tp"),
        ),
        check_vma=False,
    )
```

```python
import functools

import jax
import jax.numpy as jnp
from jax import lax
from jax.experimental import pallas as pl
from jax.experimental.pallas import tpu as pltpu
from jax.sharding import PartitionSpec as P

MESH = pl.DeviceIdType.MESH
F32 = jnp.float32
BF16 = jnp.bfloat16
epsilon = 1e-06
LANES = 128
BLOCKS = 8
HIGH = lax.Precision.HIGHEST
LAST = (((1,), (1,)), ((), ()))


def far_first(count):
    return sorted(range(1, count), key=lambda o: -min(o, count - o))


def silu(z):
    return z / (1.0 + jnp.exp(-z))


def high_part(v):
    return v.astype(BF16).astype(F32)


def wait_bytes(ref, sem):
    pltpu.make_async_copy(ref, ref, sem).wait()


def lane_rows(block, first):
    return jnp.concatenate([block[first : first + 1], block[first + 1 : first + 2]], axis=1)


def flush(*refs):
    count = len(refs) // 2
    sems = refs[-1]
    copies = [pltpu.make_async_copy(refs[i], refs[count + i], sems.at[i]) for i in range(count)]
    for c in copies:
        c.start()
    for c in copies:
        c.wait()


def kernel(n_dp, n_tp, *refs):
    given, rest = refs[:21], refs[21:]
    outs, held, rest = rest[:5], rest[5:25], rest[25:]
    scratch, in_sem = rest[:-1], rest[-1]
    state_in = given[17]
    whole = [g for i, g in enumerate(given) if i != 17]
    barrier = pltpu.get_barrier_semaphore()
    dp, tp = lax.axis_index("dp"), lax.axis_index("tp")
    state = scratch[15]
    loads = [pltpu.make_async_copy(g, h, in_sem.at[i]) for i, (g, h) in enumerate(zip(whole, held))]
    loads.append(pltpu.make_async_copy(state_in, state, in_sem.at[len(whole)]))
    for c in loads[:9]:
        c.start()
    for o in far_first(n_dp):
        pl.semaphore_signal(barrier, inc=1, device_id={"dp": lax.rem(dp + o, n_dp)}, device_id_type=MESH)
    for c in loads[9:]:
        c.start()
    for o in far_first(n_tp):
        pl.semaphore_signal(barrier, inc=1, device_id={"tp": lax.rem(tp + o, n_tp)}, device_id_type=MESH)
    body(n_dp, n_tp, barrier, loads, *held, *outs, *scratch)


def body(
    n_dp,
    n_tp,
    barrier,
    loads,
    hidden,
    lengths,
    in_gain,
    w_gate,
    w_value,
    w_write,
    w_read,
    w_step,
    step_bias,
    log_rate,
    direct_gain,
    taps_value,
    taps_write,
    taps_read,
    log_decay,
    group_gain,
    w_out,
    hist_value,
    hist_write,
    hist_read,
    stream_out,
    state_new,
    buf_value,
    buf_write,
    buf_read,
    part,
    rs_send,
    rs_recv,
    rs_half_send,
    rs_half_recv,
    ag_send,
    ag_half_recv,
    ag_recv,
    gathered,
    ar_send,
    ar_recv,
    w_pair,
    w_pair_out,
    x_mine,
    x_other,
    state,
    state_hi,
    state_lo,
    w_pack,
    conv_base,
    conv_last,
    decay_pad,
    head_pad,
    o_gate,
    o_value,
    o_write,
    o_read,
    o_step,
    o_out,
    o_gain,
    o_hidden,
    swap_ssem,
    swap_rsem,
    rs_ssem,
    rs_rsem,
    ag_ssem,
    ag_rsem,
    ar_ssem,
    ar_rsem,
):
    dp, tp = lax.axis_index("dp"), lax.axis_index("tp")
    layers, feats = in_gain.shape
    seqs = hidden.shape[0]
    width = feats * n_dp
    heads = step_bias.shape[1]
    inner = w_gate.shape[2]
    head_dim = inner // heads
    depth = hist_value.shape[1]
    half = seqs // 2

    lane_inner = lax.broadcasted_iota(jnp.int32, (2, inner), 1)
    pick = (
        lax.broadcasted_iota(jnp.int32, (w_step.shape[2], LANES), 0)
        == lax.broadcasted_iota(jnp.int32, (w_step.shape[2], LANES), 1) + tp * heads
    ) & (lax.broadcasted_iota(jnp.int32, (w_step.shape[2], LANES), 1) < heads)
    pick = pick.astype(F32).astype(BF16)

    def per_head(rows):
        out = jnp.broadcast_to(rows[:, heads - 1 : heads], (rows.shape[0], inner))
        lane = lane_inner[: rows.shape[0]]
        for h in range(heads - 2, -1, -1):
            out = jnp.where(lane < (h + 1) * head_dim, rows[:, h : h + 1], out)
        return out

    def lay_out(columns, count):
        for c, column in enumerate(columns):
            part[pl.ds(c, count, stride=BLOCKS), :] = column
        return part[0 : count * BLOCKS, :].reshape(count // 2, 2 * BLOCKS, LANES).astype(BF16)

    def with_rest(columns, step, square):
        lane = lax.broadcasted_iota(jnp.int32, step.shape, 1)
        rest = jnp.where(lane == heads, square, step)
        high = high_part(rest)
        return columns + [high, rest - high]

    def cut(r):
        return [r[:, at : at + LANES] for at in range(0, r.shape[1], LANES)]

    def send(src, dst, ssem, rsem, **to):
        pltpu.make_async_remote_copy(
            src_ref=src, dst_ref=dst, send_sem=ssem, recv_sem=rsem, device_id=to, device_id_type=MESH
        ).start()

    chip, core = dp // 2, lax.rem(dp, 2)
    chips = n_dp // 2
    sibling = dp + 1 - 2 * core
    my_half, my_place = dp // chips, lax.rem(dp, chips)
    served_here = my_half == core

    def wait_half(ref, sem):
        @pl.when(served_here)
        def _():
            wait_bytes(ref.at[pl.ds(0, chips - 1)], sem)

        @pl.when(jnp.logical_not(served_here))
        def _():
            wait_bytes(ref, sem)

    def send_branch(l):
        for o in far_first(n_tp):
            send(ar_send.at[l], ar_recv.at[l, tp], ar_ssem.at[l], ar_rsem.at[l], tp=lax.rem(tp + o, n_tp))
        ar_recv[l, tp] = ar_send[l]

    for c in loads[:8]:
        c.wait()
    x_bf = hidden[...]
    x = x_bf.astype(F32)
    normed = (x * in_gain[0:1, :]).astype(BF16)
    columns = []
    for w in (w_gate, w_value, w_write, w_read):
        columns += cut(jnp.dot(normed, w[0], preferred_element_type=F32))
    w_mine = jnp.dot(w_step[0], pick, preferred_element_type=F32).astype(BF16)
    step = jnp.dot(normed, w_mine, preferred_element_type=F32)
    rs_send[...] = lay_out(with_rest(columns, step, jnp.sum(x * x, axis=1, keepdims=True)), seqs)

    for c in loads[8:]:
        c.wait()
    position = [lengths[s] - 1 for s in range(2)]
    row8 = lax.broadcasted_iota(jnp.int32, (8, log_decay.shape[2]), 0)
    lane_pos = lax.broadcasted_iota(jnp.int32, (8, log_decay.shape[2]), 1)
    at_position = (lane_pos == jnp.where(row8 == 0, position[0], position[1])).astype(F32)
    row2 = lax.broadcasted_iota(jnp.int32, (2, LANES), 0)
    is_live = jnp.where(jnp.where(row2 == 0, position[0], position[1]) > 0, 1.0, 0.0)
    conv_base[...] = jnp.zeros_like(conv_base)
    conv_last[...] = jnp.zeros_like(conv_last)
    decay_pad[...] = jnp.zeros_like(decay_pad)
    head_pad[...] = jnp.zeros_like(head_pad)
    w_pack[...] = jnp.zeros_like(w_pack)
    w_pack[0:feats, 0:inner] = w_out[1]
    w_pack[feats : 2 * feats, inner : 2 * inner] = w_out[1]

    def keep_pair(first, gate, value, write, read, step, out):
        at, to = slice(first, first + feats), 0
        mine = jnp.dot(step, pick, preferred_element_type=F32).astype(BF16)
        for w in (gate, value, write, read, mine):
            w_pair[at, to : to + w.shape[1]] = w
            to += w.shape[1]
        w_pair_out[at, :] = out

    keep_pair(0, w_gate[1], w_value[1], w_write[1], w_read[1], w_step[1], w_out[0])
    decay_log = []
    for l in range(layers):
        decay_pad[l, 0:heads, :] = log_decay[l]
        picked = lax.dot_general(at_position, decay_pad[l], LAST, precision=HIGH, preferred_element_type=F32)
        decay_log.append(picked[0:2])
        head_pad[l, 0:1, 0:heads] = step_bias[l : l + 1, :]
        head_pad[l, 1:2, 0:heads] = jnp.exp(log_rate[l : l + 1, :])
        for taps, hist, row in (
            (taps_value, hist_value, 2),
            (taps_write, hist_write, 4),
            (taps_read, hist_read, 5),
        ):
            tap = taps[l].astype(F32)
            total = None
            for k in range(depth):
                rows = hist[l, k].astype(F32)
                valid = jnp.where(
                    lax.broadcasted_iota(jnp.int32, rows.shape, 0) == 0,
                    jnp.where(k >= depth - position[0], 1.0, 0.0),
                    jnp.where(k >= depth - position[1], 1.0, 0.0),
                )
                term = rows * tap[k : k + 1] * valid
                total = term if total is None else total + term
            for c in range(rows.shape[1] // LANES):
                for s in range(2):
                    at = s * BLOCKS + row + c
                    conv_base[l, at : at + 1, :] = total[s : s + 1, c * LANES : (c + 1) * LANES]
                    conv_last[l, at : at + 1, :] = tap[depth : depth + 1, c * LANES : (c + 1) * LANES]
    for l in range(layers):
        high = state[l].astype(BF16)
        state_hi[l] = high
        state_lo[l] = (state[l] - high.astype(F32)).astype(BF16)

    pl.semaphore_wait(barrier, n_dp - 1 + n_tp - 1)

    row16 = lax.broadcasted_iota(jnp.int32, (2 * BLOCKS, LANES), 0)
    is_gate = lax.rem(row16, BLOCKS) < 2
    row_of8 = lax.broadcasted_iota(jnp.int32, (8, LANES), 0)
    assert layers == 2
    for l in range(layers):
        if l == 0:
            for o in far_first(n_dp):
                to = lax.rem(dp + o, n_dp)
                send(rs_send.at[to], rs_recv.at[dp], rs_ssem.at[l], rs_rsem.at[l], dp=to)
            rs_recv[dp] = rs_send[dp]
            swaps = (
                (w_gate.at[1], o_gate),
                (w_value.at[1], o_value),
                (w_write.at[1], o_write),
                (w_read.at[1], o_read),
                (w_step.at[1], o_step),
                (w_out.at[0], o_out),
                (in_gain, o_gain),
                (hidden, o_hidden),
            )
            for i, (src, dst) in enumerate(swaps):
                send(src, dst, swap_ssem.at[i], swap_rsem.at[i], dp=sibling)
            wait_bytes(rs_recv.at[pl.ds(0, n_dp - 1)], rs_rsem.at[l])
            received = rs_recv[...]
        else:

            @pl.when(jnp.logical_not(served_here))
            def _():
                send(
                    rs_half_send.at[my_place],
                    rs_half_recv.at[chip],
                    rs_ssem.at[1],
                    rs_rsem.at[1],
                    dp=core * chips + my_place,
                )

            @pl.when(served_here)
            def _():
                rs_half_recv[chip] = rs_half_send[my_place]

            for o in far_first(chips):
                to = lax.rem(my_place + o, chips)
                send(rs_half_send.at[to], rs_half_recv.at[chip], rs_ssem.at[l], rs_rsem.at[l], dp=core * chips + to)
            send(x_mine, x_other, swap_ssem.at[8], swap_rsem.at[8], dp=sibling)
            wait_half(rs_half_recv, rs_rsem.at[l])
            received = rs_half_recv[...]
        summed = jnp.sum(received.astype(F32), axis=0)
        rest = jnp.concatenate(
            [summed[BLOCKS * s + 6 : BLOCKS * s + 7] + summed[BLOCKS * s + 7 : BLOCKS * s + 8] for s in range(2)], axis=0
        )
        row_scale = lax.rsqrt(rest[:, heads : heads + 1] / width + epsilon)
        scale16 = jnp.where(row16 < BLOCKS, row_scale[0:1], row_scale[1:2])
        scaled = summed * scale16
        current = high_part(scaled)
        act = silu(jnp.where(is_gate, scaled, conv_base[l] + current * conv_last[l]))
        z = rest * row_scale + head_pad[l, 0:1, :]
        step = jnp.maximum(z, 0.0) + jnp.log1p(jnp.exp(-jnp.abs(z)))
        decay = jnp.exp(decay_log[l] - head_pad[l, 1:2, :] * step) * is_live
        gate_row = jnp.concatenate([lane_rows(act, BLOCKS * s) for s in range(2)], axis=0)
        value_row = jnp.concatenate([lane_rows(act, BLOCKS * s + 2) for s in range(2)], axis=0)
        step_value = per_head(step) * value_row
        decay_row = per_head(decay)
        readout, along = [], []
        for s in range(2):
            write = act[BLOCKS * s + 4 : BLOCKS * s + 5]
            read = act[BLOCKS * s + 5 : BLOCKS * s + 6]
            high = high_part(read)
            lhs = jnp.where(row_of8 == 0, high, jnp.where(row_of8 == 1, read - high, 0.0)).astype(BF16)
            a = lax.dot_general(lhs, state_hi[l, s], LAST, preferred_element_type=F32)
            b = lax.dot_general(lhs, state_lo[l, s], LAST, preferred_element_type=F32)
            readout.append(a[0:1] + a[1:2] + b[0:1])
            along.append(jnp.sum(write * read, axis=1, keepdims=True))
        readout = jnp.concatenate(readout, axis=0)
        along = jnp.concatenate(along, axis=0)
        mixed = (
            decay_row * readout + step_value * along + per_head(direct_gain[l : l + 1, :]) * value_row
        ) * gate_row
        mean = jnp.sum(mixed * mixed, axis=1, keepdims=True) / inner
        gated = mixed * lax.rsqrt(mean + epsilon) * group_gain[l : l + 1, :]
        ag_send[l] = gated.astype(BF16)
        if l == 0:
            for o in far_first(chips):
                to = 2 * lax.rem(chip + o, chips) + my_half
                send(ag_send.at[l], ag_half_recv.at[my_place], ag_ssem.at[l], ag_rsem.at[l], dp=to)

            @pl.when(jnp.logical_not(served_here))
            def _():
                send(ag_send.at[0], ag_half_recv.at[my_place], ag_ssem.at[0], ag_rsem.at[0], dp=sibling)

            @pl.when(served_here)
            def _():
                ag_half_recv[my_place] = ag_send[0]
        else:
            for o in far_first(n_dp):
                send(ag_send.at[l], ag_recv.at[dp], ag_ssem.at[l], ag_rsem.at[l], dp=lax.rem(dp + o, n_dp))
            ag_recv[dp] = ag_send[l]

        for b in range(inner // LANES):
            cols = jnp.transpose(
                jnp.concatenate(
                    [step_value[:, b * LANES : (b + 1) * LANES], jnp.zeros((6, LANES), F32)], axis=0
                )
            )
            for s in range(2):
                write = act[BLOCKS * s + 4 : BLOCKS * s + 5]
                for j in range(LANES // head_dim):
                    h = b * (LANES // head_dim) + j
                    at = slice(h * head_dim, (h + 1) * head_dim)
                    state_new[l, s, at, :] = (
                        decay[s : s + 1, h : h + 1] * state[l, s, at, :]
                        + cols[j * head_dim : (j + 1) * head_dim, s : s + 1] * write
                    )
        for k in range(depth - 1):
            buf_value[l, k] = hist_value[l, k + 1]
            buf_write[l, k] = hist_write[l, k + 1]
            buf_read[l, k] = hist_read[l, k + 1]
        buf_value[l, depth - 1] = jnp.concatenate(
            [lane_rows(current, BLOCKS * s + 2) for s in range(2)], axis=0
        ).astype(BF16)
        buf_write[l, depth - 1] = jnp.concatenate(
            [current[BLOCKS * s + 4 : BLOCKS * s + 5] for s in range(2)], axis=0
        ).astype(BF16)
        buf_read[l, depth - 1] = jnp.concatenate(
            [current[BLOCKS * s + 5 : BLOCKS * s + 6] for s in range(2)], axis=0
        ).astype(BF16)

        half_rows = pl.ds(pl.multiple_of(core * half, half), half)
        if l == 0:
            for i, (src, dst) in enumerate(swaps):
                pltpu.make_async_copy(dst, dst, swap_rsem.at[i]).wait()
            keep_pair(feats, o_gate[...], o_value[...], o_write[...], o_read[...], o_step[...], o_out[...])
            pair_gain = jnp.concatenate([in_gain[1:2, :], o_gain[1:2, :]], axis=1)
            x = jnp.concatenate([hidden[half_rows, :].astype(F32), o_hidden[half_rows, :].astype(F32)], axis=1)
            wait_half(ag_half_recv, ag_rsem.at[l])
            for d in range(chips):
                gathered[2 * d : 2 * d + 2, :] = ag_half_recv[d].astype(F32)
            rows, weight = gathered[0:half, :].astype(BF16), w_pair_out[...]
        else:
            wait_bytes(x_other, swap_rsem.at[8])
            mine, other = x[:, :feats], x_other[...].astype(F32)[:, feats:]
            is_first = core == 0
            x = jnp.concatenate([jnp.where(is_first, mine, other), jnp.where(is_first, other, mine)], axis=1)
            wait_bytes(ag_recv.at[pl.ds(0, n_dp - 1)], ag_rsem.at[l])
            for d in range(n_dp):
                gathered[2 * d : 2 * d + 2, :] = ag_recv[d].astype(F32)
            rows = jnp.concatenate([gathered[0:half, :], gathered[half:, :]], axis=1).astype(BF16)
            weight = w_pack[...]
        ar_send[l] = lax.dot_general(rows, weight, LAST, preferred_element_type=F32).astype(BF16)
        send_branch(l)
        wait_bytes(ar_recv.at[l, pl.ds(0, n_tp - 1)], ar_rsem.at[l])
        x = high_part(x + jnp.sum(ar_recv[l].astype(F32), axis=0))
        if l == 0:
            normed = (x * pair_gain).astype(BF16)
            columns = cut(jnp.dot(normed, w_pair[...], preferred_element_type=F32))
            step = columns.pop()
            rs_half_send[...] = lay_out(with_rest(columns, step, jnp.sum(x * x, axis=1, keepdims=True)), half)
            x_mine[...] = x.astype(BF16)
    stream_out[...] = jnp.concatenate([x[:, :feats], x[:, feats:]], axis=0).astype(BF16)
    wait_bytes(rs_send.at[pl.ds(0, n_dp - 1)], rs_ssem.at[0])
    wait_half(rs_half_send, rs_ssem.at[1])
    wait_half(ag_half_recv, ag_ssem.at[0])
    wait_bytes(ag_recv.at[pl.ds(0, n_dp - 1)], ag_ssem.at[1])
    for l in range(layers):
        wait_bytes(ar_recv.at[l, pl.ds(0, n_tp - 1)], ar_ssem.at[l])
    for i, (src, dst) in enumerate(swaps):
        pltpu.make_async_copy(src, src, swap_ssem.at[i]).wait()
    wait_bytes(x_mine, swap_ssem.at[8])


def on_device(
    hidden,
    lengths,
    input_norm_gain,
    gate_matrix,
    input_matrix,
    write_matrix,
    read_matrix,
    step_matrix,
    step_size_bias,
    log_decay_rate,
    direct_path_gain,
    input_filter_taps,
    write_filter_taps,
    read_filter_taps,
    position_log_decay,
    grouped_norm_gain,
    output_matrix,
    recurrent_head_state,
    history_input_rows,
    history_write_rows,
    history_read_rows,
):
    n_dp, n_tp = lax.axis_size("dp"), lax.axis_size("tp")
    layers, seq_local, heads, head_dim, state_dim = recurrent_head_state.shape
    inner = heads * head_dim
    seqs, feats = hidden.shape
    assert seq_local == 2 and state_dim == LANES and write_matrix.shape[2] == LANES and inner == 2 * LANES
    state_shape = (layers, seq_local, inner, state_dim)
    operands = (
        hidden,
        lengths,
        input_norm_gain,
        gate_matrix,
        input_matrix,
        write_matrix,
        read_matrix,
        step_matrix,
        step_size_bias,
        log_decay_rate,
        direct_path_gain,
        input_filter_taps,
        write_filter_taps,
        read_filter_taps,
        position_log_decay.transpose(0, 2, 1),
        grouped_norm_gain,
        output_matrix.transpose(0, 2, 1),
        recurrent_head_state.reshape(state_shape),
        history_input_rows.transpose(0, 2, 1, 3),
        history_write_rows.transpose(0, 2, 1, 3),
        history_read_rows.transpose(0, 2, 1, 3),
    )
    vmem, hbm = pl.BlockSpec(memory_space=pltpu.VMEM), pl.BlockSpec(memory_space=pltpu.HBM)
    in_specs = [hbm] * len(operands)
    results = [operands[i] for i in (0, 17, 18, 19, 20)]
    positions = position_log_decay.shape[1]
    dma = pltpu.SemaphoreType.DMA
    whole = [o for i, o in enumerate(operands) if i != 17]
    space = lambda o: pltpu.SMEM if o is lengths else pltpu.VMEM
    finished = pl.pallas_call(
        functools.partial(kernel, n_dp, n_tp),
        out_shape=[pltpu.VMEM(r.shape, r.dtype) for r in results],
        in_specs=in_specs,
        out_specs=[vmem] * len(results),
        scratch_shapes=[space(o)(o.shape, o.dtype) for o in whole]
        + [
            pltpu.VMEM((seqs * BLOCKS, LANES), F32),
            pltpu.VMEM((n_dp, 2 * BLOCKS, LANES), BF16),
            pltpu.VMEM((n_dp, 2 * BLOCKS, LANES), BF16),
            pltpu.VMEM((n_dp // 2, 2 * BLOCKS, LANES), BF16),
            pltpu.VMEM((n_dp // 2, 2 * BLOCKS, LANES), BF16),
            pltpu.VMEM((layers, 2, inner), BF16),
            pltpu.VMEM((n_dp // 2, 2, inner), BF16),
            pltpu.VMEM((n_dp, 2, inner), BF16),
            pltpu.VMEM((seqs, inner), F32),
            pltpu.VMEM((layers, seqs // 2, 2 * feats), BF16),
            pltpu.VMEM((layers, n_tp, seqs // 2, 2 * feats), BF16),
            pltpu.VMEM((2 * feats, 7 * LANES), BF16),
            pltpu.VMEM((2 * feats, inner), BF16),
            pltpu.VMEM((seqs // 2, 2 * feats), BF16),
            pltpu.VMEM((seqs // 2, 2 * feats), BF16),
            pltpu.VMEM(state_shape, F32),
            pltpu.VMEM(state_shape, BF16),
            pltpu.VMEM(state_shape, BF16),
            pltpu.VMEM((2 * feats, 2 * inner), BF16),
            pltpu.VMEM((layers, 2 * BLOCKS, LANES), F32),
            pltpu.VMEM((layers, 2 * BLOCKS, LANES), F32),
            pltpu.VMEM((layers, LANES, positions), F32),
            pltpu.VMEM((layers, 8, LANES), F32),
        ]
        + [pltpu.VMEM(o.shape[1:], o.dtype) for o in (gate_matrix, input_matrix, write_matrix, read_matrix, step_matrix)]
        + [
            pltpu.VMEM(operands[16].shape[1:], BF16),
            pltpu.VMEM(input_norm_gain.shape, F32),
            pltpu.VMEM(hidden.shape, BF16),
            dma((9,)),
            dma((9,)),
        ]
        + [dma((layers,))] * 6
        + [dma((len(whole) + 1,))],
        compiler_params=pltpu.CompilerParams(
            collective_id=0, has_side_effects=True
        ),
        name="mixers",
    )(*operands)
    stream, states, values, writes, reads = pl.pallas_call(
        flush,
        out_shape=[jax.ShapeDtypeStruct(r.shape, r.dtype) for r in results],
        in_specs=[vmem] * len(results),
        out_specs=[hbm] * len(results),
        scratch_shapes=[dma((len(results),))],
        compiler_params=pltpu.CompilerParams(vmem_limit_bytes=4 * 1024 * 1024),
        name="flush",
    )(*finished)
    return (
        stream,
        states.reshape(recurrent_head_state.shape),
        values.transpose(0, 2, 1, 3),
        writes.transpose(0, 2, 1, 3),
        reads.transpose(0, 2, 1, 3),
    )


def solution(mesh):
    placed = (
        P("grp", "dp"),
        P(("grp", "dp")),
        P(None, "dp"),
        P(None, "dp", "tp"),
        P(None, "dp", "tp"),
        P(None, "dp", "tp"),
        P(None, "dp", "tp"),
        P(None, "dp", None),
        P(None, "tp"),
        P(None, "tp"),
        P(None, "tp"),
        P(None, None, "tp"),
        P(None, None, "tp"),
        P(None, None, "tp"),
        P(None, None, "tp"),
        P(None, "tp"),
        P(None, "tp", "dp"),
        P(None, ("grp", "dp"), "tp", None, None),
        P(None, ("grp", "dp"), None, "tp"),
        P(None, ("grp", "dp"), None, "tp"),
        P(None, ("grp", "dp"), None, "tp"),
    )
    return jax.shard_map(
        on_device,
        mesh=mesh,
        in_specs=placed,
        out_specs=(
            P("grp", "dp"),
            P(None, ("grp", "dp"), "tp", None, None),
            P(None, ("grp", "dp"), None, "tp"),
            P(None, ("grp", "dp"), None, "tp"),
            P(None, ("grp", "dp"), None, "tp"),
        ),
        check_vma=False,
    )
```

```python
import functools

import jax
import jax.numpy as jnp
from jax import lax
from jax.experimental import pallas as pl
from jax.experimental.pallas import tpu as pltpu
from jax.sharding import PartitionSpec as P

MESH = pl.DeviceIdType.MESH
F32 = jnp.float32
BF16 = jnp.bfloat16
epsilon = 1e-06
LANES = 128
BLOCKS = 8
HIGH = lax.Precision.HIGHEST
LAST = (((1,), (1,)), ((), ()))


def far_first(count):
    return sorted(range(1, count), key=lambda o: -min(o, count - o))


def silu(z):
    return z / (1.0 + jnp.exp(-z))


def high_part(v):
    return v.astype(BF16).astype(F32)


def wait_bytes(ref, sem):
    pltpu.make_async_copy(ref, ref, sem).wait()


def lane_rows(block, first):
    return jnp.concatenate([block[first : first + 1], block[first + 1 : first + 2]], axis=1)


def flush(*refs):
    count = len(refs) // 2
    sems = refs[-1]
    copies = [pltpu.make_async_copy(refs[i], refs[count + i], sems.at[i]) for i in range(count)]
    for c in copies:
        c.start()
    for c in copies:
        c.wait()


def kernel(n_dp, n_tp, *refs):
    given, rest = refs[:21], refs[21:]
    outs, held, rest = rest[:5], rest[5:25], rest[25:]
    scratch, in_sem = rest[:-1], rest[-1]
    state_in = given[17]
    whole = [g for i, g in enumerate(given) if i != 17]
    barrier = pltpu.get_barrier_semaphore()
    dp, tp = lax.axis_index("dp"), lax.axis_index("tp")
    state = scratch[15]
    loads = [pltpu.make_async_copy(g, h, in_sem.at[i]) for i, (g, h) in enumerate(zip(whole, held))]
    loads.append(pltpu.make_async_copy(state_in, state, in_sem.at[len(whole)]))
    for c in loads[:9]:
        c.start()
    for o in far_first(n_dp):
        pl.semaphore_signal(barrier, inc=1, device_id={"dp": lax.rem(dp + o, n_dp)}, device_id_type=MESH)
    for c in loads[9:]:
        c.start()
    for z in range(n_tp - 1, 0, -1):

        @pl.when(z > tp)
        def _(z=z):
            pl.semaphore_signal(barrier, inc=1, device_id={"tp": z}, device_id_type=MESH)

    body(n_dp, n_tp, barrier, loads, *held, *outs, *scratch)


def body(
    n_dp,
    n_tp,
    barrier,
    loads,
    hidden,
    lengths,
    in_gain,
    w_gate,
    w_value,
    w_write,
    w_read,
    w_step,
    step_bias,
    log_rate,
    direct_gain,
    taps_value,
    taps_write,
    taps_read,
    log_decay,
    group_gain,
    w_out,
    hist_value,
    hist_write,
    hist_read,
    stream_out,
    state_new,
    buf_value,
    buf_write,
    buf_read,
    part,
    rs_send,
    rs_recv,
    rs_half_send,
    rs_half_recv,
    ag_send,
    ag_half_recv,
    ag_recv,
    gathered,
    ar_send,
    ar_recv,
    w_pair,
    w_pair_out,
    x_mine,
    x_other,
    state,
    state_hi,
    state_lo,
    w_pack,
    conv_base,
    conv_last,
    decay_pad,
    head_pad,
    o_gate,
    o_value,
    o_write,
    o_read,
    o_step,
    o_out,
    o_gain,
    o_hidden,
    swap_ssem,
    swap_rsem,
    rs_ssem,
    rs_rsem,
    ag_ssem,
    ag_rsem,
    ar_ssem,
    ar_rsem,
    entered,
):
    dp, tp = lax.axis_index("dp"), lax.axis_index("tp")
    layers, feats = in_gain.shape
    seqs = hidden.shape[0]
    width = feats * n_dp
    heads = step_bias.shape[1]
    inner = w_gate.shape[2]
    head_dim = inner // heads
    depth = hist_value.shape[1]
    half = seqs // 2

    lane_inner = lax.broadcasted_iota(jnp.int32, (2, inner), 1)
    pick = (
        lax.broadcasted_iota(jnp.int32, (w_step.shape[2], LANES), 0)
        == lax.broadcasted_iota(jnp.int32, (w_step.shape[2], LANES), 1) + tp * heads
    ) & (lax.broadcasted_iota(jnp.int32, (w_step.shape[2], LANES), 1) < heads)
    pick = pick.astype(F32).astype(BF16)

    def per_head(rows):
        out = jnp.broadcast_to(rows[:, heads - 1 : heads], (rows.shape[0], inner))
        lane = lane_inner[: rows.shape[0]]
        for h in range(heads - 2, -1, -1):
            out = jnp.where(lane < (h + 1) * head_dim, rows[:, h : h + 1], out)
        return out

    def lay_out(columns, count):
        for c, column in enumerate(columns):
            part[pl.ds(c, count, stride=BLOCKS), :] = column
        return part[0 : count * BLOCKS, :].reshape(count // 2, 2 * BLOCKS, LANES).astype(BF16)

    def with_rest(columns, step, square):
        lane = lax.broadcasted_iota(jnp.int32, step.shape, 1)
        rest = jnp.where(lane == heads, square, step)
        high = high_part(rest)
        return columns + [high, rest - high]

    def cut(r):
        return [r[:, at : at + LANES] for at in range(0, r.shape[1], LANES)]

    def send(src, dst, ssem, rsem, **to):
        pltpu.make_async_remote_copy(
            src_ref=src, dst_ref=dst, send_sem=ssem, recv_sem=rsem, device_id=to, device_id_type=MESH
        ).start()

    chip, core = dp // 2, lax.rem(dp, 2)
    chips = n_dp // 2
    sibling = dp + 1 - 2 * core
    my_half, my_place = dp // chips, lax.rem(dp, chips)
    served_here = my_half == core

    def wait_half(ref, sem):
        @pl.when(served_here)
        def _():
            wait_bytes(ref.at[pl.ds(0, chips - 1)], sem)

        @pl.when(jnp.logical_not(served_here))
        def _():
            wait_bytes(ref, sem)

    def send_branch(l):
        for o in far_first(n_tp):
            send(ar_send.at[l], ar_recv.at[l, tp], ar_ssem.at[l], ar_rsem.at[l], tp=lax.rem(tp + o, n_tp))
        ar_recv[l, tp] = ar_send[l]

    for c in loads[:8]:
        c.wait()
    x_bf = hidden[...]
    x = x_bf.astype(F32)
    normed = (x * in_gain[0:1, :]).astype(BF16)
    columns = []
    for w in (w_gate, w_value, w_write, w_read):
        columns += cut(jnp.dot(normed, w[0], preferred_element_type=F32))
    w_mine = jnp.dot(w_step[0], pick, preferred_element_type=F32).astype(BF16)
    step = jnp.dot(normed, w_mine, preferred_element_type=F32)
    rs_send[...] = lay_out(with_rest(columns, step, jnp.sum(x * x, axis=1, keepdims=True)), seqs)

    for c in loads[8:]:
        c.wait()
    position = [lengths[s] - 1 for s in range(2)]
    row8 = lax.broadcasted_iota(jnp.int32, (8, log_decay.shape[2]), 0)
    lane_pos = lax.broadcasted_iota(jnp.int32, (8, log_decay.shape[2]), 1)
    at_position = (lane_pos == jnp.where(row8 == 0, position[0], position[1])).astype(F32)
    row2 = lax.broadcasted_iota(jnp.int32, (2, LANES), 0)
    is_live = jnp.where(jnp.where(row2 == 0, position[0], position[1]) > 0, 1.0, 0.0)
    conv_base[...] = jnp.zeros_like(conv_base)
    conv_last[...] = jnp.zeros_like(conv_last)
    decay_pad[...] = jnp.zeros_like(decay_pad)
    head_pad[...] = jnp.zeros_like(head_pad)
    w_pack[...] = jnp.zeros_like(w_pack)
    w_pack[0:feats, 0:inner] = w_out[1]
    w_pack[feats : 2 * feats, inner : 2 * inner] = w_out[1]

    def keep_pair(first, gate, value, write, read, step, out):
        at, to = slice(first, first + feats), 0
        mine = jnp.dot(step, pick, preferred_element_type=F32).astype(BF16)
        for w in (gate, value, write, read, mine):
            w_pair[at, to : to + w.shape[1]] = w
            to += w.shape[1]
        w_pair_out[at, :] = out

    keep_pair(0, w_gate[1], w_value[1], w_write[1], w_read[1], w_step[1], w_out[0])
    decay_log = []
    for l in range(layers):
        decay_pad[l, 0:heads, :] = log_decay[l]
        picked = lax.dot_general(at_position, decay_pad[l], LAST, precision=HIGH, preferred_element_type=F32)
        decay_log.append(picked[0:2])
        head_pad[l, 0:1, 0:heads] = step_bias[l : l + 1, :]
        head_pad[l, 1:2, 0:heads] = jnp.exp(log_rate[l : l + 1, :])
        for taps, hist, row in (
            (taps_value, hist_value, 2),
            (taps_write, hist_write, 4),
            (taps_read, hist_read, 5),
        ):
            tap = taps[l].astype(F32)
            total = None
            for k in range(depth):
                rows = hist[l, k].astype(F32)
                valid = jnp.where(
                    lax.broadcasted_iota(jnp.int32, rows.shape, 0) == 0,
                    jnp.where(k >= depth - position[0], 1.0, 0.0),
                    jnp.where(k >= depth - position[1], 1.0, 0.0),
                )
                term = rows * tap[k : k + 1] * valid
                total = term if total is None else total + term
            for c in range(rows.shape[1] // LANES):
                for s in range(2):
                    at = s * BLOCKS + row + c
                    conv_base[l, at : at + 1, :] = total[s : s + 1, c * LANES : (c + 1) * LANES]
                    conv_last[l, at : at + 1, :] = tap[depth : depth + 1, c * LANES : (c + 1) * LANES]
    for l in range(layers):
        high = state[l].astype(BF16)
        state_hi[l] = high
        state_lo[l] = (state[l] - high.astype(F32)).astype(BF16)

    pl.semaphore_wait(barrier, n_dp - 1 + tp)

    row16 = lax.broadcasted_iota(jnp.int32, (2 * BLOCKS, LANES), 0)
    is_gate = lax.rem(row16, BLOCKS) < 2
    row_of8 = lax.broadcasted_iota(jnp.int32, (8, LANES), 0)
    assert layers == 2
    for l in range(layers):
        if l == 0:
            for o in far_first(n_dp):
                to = lax.rem(dp + o, n_dp)
                send(rs_send.at[to], rs_recv.at[dp], rs_ssem.at[l], rs_rsem.at[l], dp=to)
            rs_recv[dp] = rs_send[dp]
            for z in range(n_tp - 1):

                @pl.when(z < tp)
                def _(z=z):
                    pl.semaphore_signal(entered, inc=1, device_id={"tp": z}, device_id_type=MESH)

            swaps = (
                (w_gate.at[1], o_gate),
                (w_value.at[1], o_value),
                (w_write.at[1], o_write),
                (w_read.at[1], o_read),
                (w_step.at[1], o_step),
                (w_out.at[0], o_out),
                (in_gain, o_gain),
                (hidden, o_hidden),
            )
            for i, (src, dst) in enumerate(swaps):
                send(src, dst, swap_ssem.at[i], swap_rsem.at[i], dp=sibling)
            wait_bytes(rs_recv.at[pl.ds(0, n_dp - 1)], rs_rsem.at[l])
            received = rs_recv[...]
        else:

            @pl.when(jnp.logical_not(served_here))
            def _():
                send(
                    rs_half_send.at[my_place],
                    rs_half_recv.at[chip],
                    rs_ssem.at[1],
                    rs_rsem.at[1],
                    dp=core * chips + my_place,
                )

            @pl.when(served_here)
            def _():
                rs_half_recv[chip] = rs_half_send[my_place]

            for o in far_first(chips):
                to = lax.rem(my_place + o, chips)
                send(rs_half_send.at[to], rs_half_recv.at[chip], rs_ssem.at[l], rs_rsem.at[l], dp=core * chips + to)
            send(x_mine, x_other, swap_ssem.at[8], swap_rsem.at[8], dp=sibling)
            wait_half(rs_half_recv, rs_rsem.at[l])
            received = rs_half_recv[...]
        summed = jnp.sum(received.astype(F32), axis=0)
        rest = jnp.concatenate(
            [summed[BLOCKS * s + 6 : BLOCKS * s + 7] + summed[BLOCKS * s + 7 : BLOCKS * s + 8] for s in range(2)], axis=0
        )
        row_scale = lax.rsqrt(rest[:, heads : heads + 1] / width + epsilon)
        scale16 = jnp.where(row16 < BLOCKS, row_scale[0:1], row_scale[1:2])
        scaled = summed * scale16
        current = high_part(scaled)
        act = silu(jnp.where(is_gate, scaled, conv_base[l] + current * conv_last[l]))
        z = rest * row_scale + head_pad[l, 0:1, :]
        step = jnp.maximum(z, 0.0) + jnp.log1p(jnp.exp(-jnp.abs(z)))
        decay = jnp.exp(decay_log[l] - head_pad[l, 1:2, :] * step) * is_live
        gate_row = jnp.concatenate([lane_rows(act, BLOCKS * s) for s in range(2)], axis=0)
        value_row = jnp.concatenate([lane_rows(act, BLOCKS * s + 2) for s in range(2)], axis=0)
        step_value = per_head(step) * value_row
        decay_row = per_head(decay)
        readout, along = [], []
        for s in range(2):
            write = act[BLOCKS * s + 4 : BLOCKS * s + 5]
            read = act[BLOCKS * s + 5 : BLOCKS * s + 6]
            high = high_part(read)
            lhs = jnp.where(row_of8 == 0, high, jnp.where(row_of8 == 1, read - high, 0.0)).astype(BF16)
            a = lax.dot_general(lhs, state_hi[l, s], LAST, preferred_element_type=F32)
            b = lax.dot_general(lhs, state_lo[l, s], LAST, preferred_element_type=F32)
            readout.append(a[0:1] + a[1:2] + b[0:1])
            along.append(jnp.sum(write * read, axis=1, keepdims=True))
        readout = jnp.concatenate(readout, axis=0)
        along = jnp.concatenate(along, axis=0)
        mixed = (
            decay_row * readout + step_value * along + per_head(direct_gain[l : l + 1, :]) * value_row
        ) * gate_row
        mean = jnp.sum(mixed * mixed, axis=1, keepdims=True) / inner
        gated = mixed * lax.rsqrt(mean + epsilon) * group_gain[l : l + 1, :]
        ag_send[l] = gated.astype(BF16)
        if l == 0:
            for o in far_first(chips):
                to = 2 * lax.rem(chip + o, chips) + my_half
                send(ag_send.at[l], ag_half_recv.at[my_place], ag_ssem.at[l], ag_rsem.at[l], dp=to)

            @pl.when(jnp.logical_not(served_here))
            def _():
                send(ag_send.at[0], ag_half_recv.at[my_place], ag_ssem.at[0], ag_rsem.at[0], dp=sibling)

            @pl.when(served_here)
            def _():
                ag_half_recv[my_place] = ag_send[0]
        else:
            for o in far_first(n_dp):
                send(ag_send.at[l], ag_recv.at[dp], ag_ssem.at[l], ag_rsem.at[l], dp=lax.rem(dp + o, n_dp))
            ag_recv[dp] = ag_send[l]

        for b in range(inner // LANES):
            cols = jnp.transpose(
                jnp.concatenate(
                    [step_value[:, b * LANES : (b + 1) * LANES], jnp.zeros((6, LANES), F32)], axis=0
                )
            )
            for s in range(2):
                write = act[BLOCKS * s + 4 : BLOCKS * s + 5]
                for j in range(LANES // head_dim):
                    h = b * (LANES // head_dim) + j
                    at = slice(h * head_dim, (h + 1) * head_dim)
                    state_new[l, s, at, :] = (
                        decay[s : s + 1, h : h + 1] * state[l, s, at, :]
                        + cols[j * head_dim : (j + 1) * head_dim, s : s + 1] * write
                    )
        for k in range(depth - 1):
            buf_value[l, k] = hist_value[l, k + 1]
            buf_write[l, k] = hist_write[l, k + 1]
            buf_read[l, k] = hist_read[l, k + 1]
        buf_value[l, depth - 1] = jnp.concatenate(
            [lane_rows(current, BLOCKS * s + 2) for s in range(2)], axis=0
        ).astype(BF16)
        buf_write[l, depth - 1] = jnp.concatenate(
            [current[BLOCKS * s + 4 : BLOCKS * s + 5] for s in range(2)], axis=0
        ).astype(BF16)
        buf_read[l, depth - 1] = jnp.concatenate(
            [current[BLOCKS * s + 5 : BLOCKS * s + 6] for s in range(2)], axis=0
        ).astype(BF16)

        half_rows = pl.ds(pl.multiple_of(core * half, half), half)
        if l == 0:
            for i, (src, dst) in enumerate(swaps):
                pltpu.make_async_copy(dst, dst, swap_rsem.at[i]).wait()
            keep_pair(feats, o_gate[...], o_value[...], o_write[...], o_read[...], o_step[...], o_out[...])
            pair_gain = jnp.concatenate([in_gain[1:2, :], o_gain[1:2, :]], axis=1)
            x = jnp.concatenate([hidden[half_rows, :].astype(F32), o_hidden[half_rows, :].astype(F32)], axis=1)
            wait_half(ag_half_recv, ag_rsem.at[l])
            for d in range(chips):
                gathered[2 * d : 2 * d + 2, :] = ag_half_recv[d].astype(F32)
            rows, weight = gathered[0:half, :].astype(BF16), w_pair_out[...]
        else:
            wait_bytes(x_other, swap_rsem.at[8])
            mine, other = x[:, :feats], x_other[...].astype(F32)[:, feats:]
            is_first = core == 0
            x = jnp.concatenate([jnp.where(is_first, mine, other), jnp.where(is_first, other, mine)], axis=1)
            wait_bytes(ag_recv.at[pl.ds(0, n_dp - 1)], ag_rsem.at[l])
            for d in range(n_dp):
                gathered[2 * d : 2 * d + 2, :] = ag_recv[d].astype(F32)
            rows = jnp.concatenate([gathered[0:half, :], gathered[half:, :]], axis=1).astype(BF16)
            weight = w_pack[...]
        ar_send[l] = lax.dot_general(rows, weight, LAST, preferred_element_type=F32).astype(BF16)
        if l == 0:

            @pl.when(tp < n_tp - 1)
            def _():
                pl.semaphore_wait(entered, n_tp - 1 - tp)

        send_branch(l)
        wait_bytes(ar_recv.at[l, pl.ds(0, n_tp - 1)], ar_rsem.at[l])
        x = high_part(x + jnp.sum(ar_recv[l].astype(F32), axis=0))
        if l == 0:
            normed = (x * pair_gain).astype(BF16)
            columns = cut(jnp.dot(normed, w_pair[...], preferred_element_type=F32))
            step = columns.pop()
            rs_half_send[...] = lay_out(with_rest(columns, step, jnp.sum(x * x, axis=1, keepdims=True)), half)
            x_mine[...] = x.astype(BF16)
    stream_out[...] = jnp.concatenate([x[:, :feats], x[:, feats:]], axis=0).astype(BF16)
    wait_bytes(rs_send.at[pl.ds(0, n_dp - 1)], rs_ssem.at[0])
    wait_half(rs_half_send, rs_ssem.at[1])
    wait_half(ag_half_recv, ag_ssem.at[0])
    wait_bytes(ag_recv.at[pl.ds(0, n_dp - 1)], ag_ssem.at[1])
    for l in range(layers):
        wait_bytes(ar_recv.at[l, pl.ds(0, n_tp - 1)], ar_ssem.at[l])
    for i, (src, dst) in enumerate(swaps):
        pltpu.make_async_copy(src, src, swap_ssem.at[i]).wait()
    wait_bytes(x_mine, swap_ssem.at[8])


def on_device(
    hidden,
    lengths,
    input_norm_gain,
    gate_matrix,
    input_matrix,
    write_matrix,
    read_matrix,
    step_matrix,
    step_size_bias,
    log_decay_rate,
    direct_path_gain,
    input_filter_taps,
    write_filter_taps,
    read_filter_taps,
    position_log_decay,
    grouped_norm_gain,
    output_matrix,
    recurrent_head_state,
    history_input_rows,
    history_write_rows,
    history_read_rows,
):
    n_dp, n_tp = lax.axis_size("dp"), lax.axis_size("tp")
    layers, seq_local, heads, head_dim, state_dim = recurrent_head_state.shape
    inner = heads * head_dim
    seqs, feats = hidden.shape
    assert seq_local == 2 and state_dim == LANES and write_matrix.shape[2] == LANES and inner == 2 * LANES
    state_shape = (layers, seq_local, inner, state_dim)
    operands = (
        hidden,
        lengths,
        input_norm_gain,
        gate_matrix,
        input_matrix,
        write_matrix,
        read_matrix,
        step_matrix,
        step_size_bias,
        log_decay_rate,
        direct_path_gain,
        input_filter_taps,
        write_filter_taps,
        read_filter_taps,
        position_log_decay.transpose(0, 2, 1),
        grouped_norm_gain,
        output_matrix.transpose(0, 2, 1),
        recurrent_head_state.reshape(state_shape),
        history_input_rows.transpose(0, 2, 1, 3),
        history_write_rows.transpose(0, 2, 1, 3),
        history_read_rows.transpose(0, 2, 1, 3),
    )
    vmem, hbm = pl.BlockSpec(memory_space=pltpu.VMEM), pl.BlockSpec(memory_space=pltpu.HBM)
    in_specs = [hbm] * len(operands)
    results = [operands[i] for i in (0, 17, 18, 19, 20)]
    positions = position_log_decay.shape[1]
    dma = pltpu.SemaphoreType.DMA
    whole = [o for i, o in enumerate(operands) if i != 17]
    space = lambda o: pltpu.SMEM if o is lengths else pltpu.VMEM
    finished = pl.pallas_call(
        functools.partial(kernel, n_dp, n_tp),
        out_shape=[pltpu.VMEM(r.shape, r.dtype) for r in results],
        in_specs=in_specs,
        out_specs=[vmem] * len(results),
        scratch_shapes=[space(o)(o.shape, o.dtype) for o in whole]
        + [
            pltpu.VMEM((seqs * BLOCKS, LANES), F32),
            pltpu.VMEM((n_dp, 2 * BLOCKS, LANES), BF16),
            pltpu.VMEM((n_dp, 2 * BLOCKS, LANES), BF16),
            pltpu.VMEM((n_dp // 2, 2 * BLOCKS, LANES), BF16),
            pltpu.VMEM((n_dp // 2, 2 * BLOCKS, LANES), BF16),
            pltpu.VMEM((layers, 2, inner), BF16),
            pltpu.VMEM((n_dp // 2, 2, inner), BF16),
            pltpu.VMEM((n_dp, 2, inner), BF16),
            pltpu.VMEM((seqs, inner), F32),
            pltpu.VMEM((layers, seqs // 2, 2 * feats), BF16),
            pltpu.VMEM((layers, n_tp, seqs // 2, 2 * feats), BF16),
            pltpu.VMEM((2 * feats, 7 * LANES), BF16),
            pltpu.VMEM((2 * feats, inner), BF16),
            pltpu.VMEM((seqs // 2, 2 * feats), BF16),
            pltpu.VMEM((seqs // 2, 2 * feats), BF16),
            pltpu.VMEM(state_shape, F32),
            pltpu.VMEM(state_shape, BF16),
            pltpu.VMEM(state_shape, BF16),
            pltpu.VMEM((2 * feats, 2 * inner), BF16),
            pltpu.VMEM((layers, 2 * BLOCKS, LANES), F32),
            pltpu.VMEM((layers, 2 * BLOCKS, LANES), F32),
            pltpu.VMEM((layers, LANES, positions), F32),
            pltpu.VMEM((layers, 8, LANES), F32),
        ]
        + [pltpu.VMEM(o.shape[1:], o.dtype) for o in (gate_matrix, input_matrix, write_matrix, read_matrix, step_matrix)]
        + [
            pltpu.VMEM(operands[16].shape[1:], BF16),
            pltpu.VMEM(input_norm_gain.shape, F32),
            pltpu.VMEM(hidden.shape, BF16),
            dma((9,)),
            dma((9,)),
        ]
        + [dma((layers,))] * 6
        + [pltpu.SemaphoreType.REGULAR]
        + [dma((len(whole) + 1,))],
        compiler_params=pltpu.CompilerParams(
            collective_id=0, has_side_effects=True
        ),
        name="mixers",
    )(*operands)
    stream, states, values, writes, reads = pl.pallas_call(
        flush,
        out_shape=[jax.ShapeDtypeStruct(r.shape, r.dtype) for r in results],
        in_specs=[vmem] * len(results),
        out_specs=[hbm] * len(results),
        scratch_shapes=[dma((len(results),))],
        compiler_params=pltpu.CompilerParams(vmem_limit_bytes=4 * 1024 * 1024),
        name="flush",
    )(*finished)
    return (
        stream,
        states.reshape(recurrent_head_state.shape),
        values.transpose(0, 2, 1, 3),
        writes.transpose(0, 2, 1, 3),
        reads.transpose(0, 2, 1, 3),
    )


def solution(mesh):
    placed = (
        P("grp", "dp"),
        P(("grp", "dp")),
        P(None, "dp"),
        P(None, "dp", "tp"),
        P(None, "dp", "tp"),
        P(None, "dp", "tp"),
        P(None, "dp", "tp"),
        P(None, "dp", None),
        P(None, "tp"),
        P(None, "tp"),
        P(None, "tp"),
        P(None, None, "tp"),
        P(None, None, "tp"),
        P(None, None, "tp"),
        P(None, None, "tp"),
        P(None, "tp"),
        P(None, "tp", "dp"),
        P(None, ("grp", "dp"), "tp", None, None),
        P(None, ("grp", "dp"), None, "tp"),
        P(None, ("grp", "dp"), None, "tp"),
        P(None, ("grp", "dp"), None, "tp"),
    )
    return jax.shard_map(
        on_device,
        mesh=mesh,
        in_specs=placed,
        out_specs=(
            P("grp", "dp"),
            P(None, ("grp", "dp"), "tp", None, None),
            P(None, ("grp", "dp"), None, "tp"),
            P(None, ("grp", "dp"), None, "tp"),
            P(None, ("grp", "dp"), None, "tp"),
        ),
        check_vma=False,
    )
```

```python
import functools

import jax
import jax.numpy as jnp
from jax import lax
from jax.experimental import pallas as pl
from jax.experimental.pallas import tpu as pltpu
from jax.sharding import PartitionSpec as P

MESH = pl.DeviceIdType.MESH
F32 = jnp.float32
BF16 = jnp.bfloat16
epsilon = 1e-06
LANES = 128
BLOCKS = 8
HIGH = lax.Precision.HIGHEST
LAST = (((1,), (1,)), ((), ()))


def far_first(count):
    return sorted(range(1, count), key=lambda o: -min(o, count - o))


def silu(z):
    return z / (1.0 + jnp.exp(-z))


def high_part(v):
    return v.astype(BF16).astype(F32)


def wait_bytes(ref, sem):
    pltpu.make_async_copy(ref, ref, sem).wait()


def lane_rows(block, first):
    return jnp.concatenate([block[first : first + 1], block[first + 1 : first + 2]], axis=1)


def flush(*refs):
    count = len(refs) // 2
    sems = refs[-1]
    copies = [pltpu.make_async_copy(refs[i], refs[count + i], sems.at[i]) for i in range(count)]
    for c in copies:
        c.start()
    for c in copies:
        c.wait()


def kernel(n_dp, n_tp, *refs):
    given, rest = refs[:21], refs[21:]
    outs, held, rest = rest[:5], rest[5:25], rest[25:]
    scratch, in_sem = rest[:-1], rest[-1]
    state_in = given[17]
    whole = [g for i, g in enumerate(given) if i != 17]
    barrier = pltpu.get_barrier_semaphore()
    dp, tp = lax.axis_index("dp"), lax.axis_index("tp")
    state = scratch[17]
    loads = [pltpu.make_async_copy(g, h, in_sem.at[i]) for i, (g, h) in enumerate(zip(whole, held))]
    loads.append(pltpu.make_async_copy(state_in, state, in_sem.at[len(whole)]))
    for c in loads[:9]:
        c.start()
    for o in far_first(n_dp):
        pl.semaphore_signal(barrier, inc=1, device_id={"dp": lax.rem(dp + o, n_dp)}, device_id_type=MESH)
    for c in loads[9:]:
        c.start()
    for z in range(n_tp - 1, 0, -1):

        @pl.when(z > tp)
        def _(z=z):
            pl.semaphore_signal(barrier, inc=1, device_id={"tp": z}, device_id_type=MESH)

    body(n_dp, n_tp, barrier, loads, *held, *outs, *scratch)


def body(
    n_dp,
    n_tp,
    barrier,
    loads,
    hidden,
    lengths,
    in_gain,
    w_gate,
    w_value,
    w_write,
    w_read,
    w_step,
    step_bias,
    log_rate,
    direct_gain,
    taps_value,
    taps_write,
    taps_read,
    log_decay,
    group_gain,
    w_out,
    hist_value,
    hist_write,
    hist_read,
    stream_out,
    state_new,
    buf_value,
    buf_write,
    buf_read,
    part,
    rs_send,
    rs_recv,
    rs_half_send,
    rs_half_recv,
    ag_send,
    ag_half_recv,
    ag_recv,
    gathered,
    ar_send,
    ar_recv,
    w_pair,
    w_pair_out,
    x_mine,
    x_other,
    x_last,
    x_given,
    state,
    state_hi,
    state_lo,
    w_pack,
    conv_base,
    conv_last,
    decay_pad,
    head_pad,
    o_gate,
    o_value,
    o_write,
    o_read,
    o_step,
    o_out,
    o_gain,
    o_hidden,
    swap_ssem,
    swap_rsem,
    rs_ssem,
    rs_rsem,
    ag_ssem,
    ag_rsem,
    ar_ssem,
    ar_rsem,
    entered,
    last_ssem,
    last_rsem,
):
    dp, tp = lax.axis_index("dp"), lax.axis_index("tp")
    layers, feats = in_gain.shape
    seqs = hidden.shape[0]
    width = feats * n_dp
    heads = step_bias.shape[1]
    inner = w_gate.shape[2]
    head_dim = inner // heads
    depth = hist_value.shape[1]
    half = seqs // 2

    lane_inner = lax.broadcasted_iota(jnp.int32, (2, inner), 1)
    pick = (
        lax.broadcasted_iota(jnp.int32, (w_step.shape[2], LANES), 0)
        == lax.broadcasted_iota(jnp.int32, (w_step.shape[2], LANES), 1) + tp * heads
    ) & (lax.broadcasted_iota(jnp.int32, (w_step.shape[2], LANES), 1) < heads)
    pick = pick.astype(F32).astype(BF16)

    def per_head(rows):
        out = jnp.broadcast_to(rows[:, heads - 1 : heads], (rows.shape[0], inner))
        lane = lane_inner[: rows.shape[0]]
        for h in range(heads - 2, -1, -1):
            out = jnp.where(lane < (h + 1) * head_dim, rows[:, h : h + 1], out)
        return out

    def lay_out(columns, count):
        for c, column in enumerate(columns):
            part[pl.ds(c, count, stride=BLOCKS), :] = column
        return part[0 : count * BLOCKS, :].reshape(count // 2, 2 * BLOCKS, LANES).astype(BF16)

    def with_rest(columns, step, square):
        lane = lax.broadcasted_iota(jnp.int32, step.shape, 1)
        rest = jnp.where(lane == heads, square, step)
        high = high_part(rest)
        return columns + [high, rest - high]

    def cut(r):
        return [r[:, at : at + LANES] for at in range(0, r.shape[1], LANES)]

    def send(src, dst, ssem, rsem, **to):
        pltpu.make_async_remote_copy(
            src_ref=src, dst_ref=dst, send_sem=ssem, recv_sem=rsem, device_id=to, device_id_type=MESH
        ).start()

    chip, core = dp // 2, lax.rem(dp, 2)
    chips = n_dp // 2
    sibling = dp + 1 - 2 * core
    my_half, my_place = dp // chips, lax.rem(dp, chips)
    served_here = my_half == core

    def wait_half(ref, sem):
        @pl.when(served_here)
        def _():
            wait_bytes(ref.at[pl.ds(0, chips - 1)], sem)

        @pl.when(jnp.logical_not(served_here))
        def _():
            wait_bytes(ref, sem)


    for c in loads[:8]:
        c.wait()
    x_bf = hidden[...]
    x = x_bf.astype(F32)
    normed = (x * in_gain[0:1, :]).astype(BF16)
    columns = []
    for w in (w_gate, w_value, w_write, w_read):
        columns += cut(jnp.dot(normed, w[0], preferred_element_type=F32))
    w_mine = jnp.dot(w_step[0], pick, preferred_element_type=F32).astype(BF16)
    step = jnp.dot(normed, w_mine, preferred_element_type=F32)
    rs_send[...] = lay_out(with_rest(columns, step, jnp.sum(x * x, axis=1, keepdims=True)), seqs)

    for c in loads[8:]:
        c.wait()
    position = [lengths[s] - 1 for s in range(2)]
    row8 = lax.broadcasted_iota(jnp.int32, (8, log_decay.shape[2]), 0)
    lane_pos = lax.broadcasted_iota(jnp.int32, (8, log_decay.shape[2]), 1)
    at_position = (lane_pos == jnp.where(row8 == 0, position[0], position[1])).astype(F32)
    row2 = lax.broadcasted_iota(jnp.int32, (2, LANES), 0)
    is_live = jnp.where(jnp.where(row2 == 0, position[0], position[1]) > 0, 1.0, 0.0)
    conv_base[...] = jnp.zeros_like(conv_base)
    conv_last[...] = jnp.zeros_like(conv_last)
    decay_pad[...] = jnp.zeros_like(decay_pad)
    head_pad[...] = jnp.zeros_like(head_pad)
    w_pack[...] = jnp.zeros_like(w_pack)
    w_pack[0:feats, 0:inner] = w_out[1]
    w_pack[feats : 2 * feats, inner : 2 * inner] = w_out[1]

    def keep_pair(first, gate, value, write, read, step, out):
        at, to = slice(first, first + feats), 0
        mine = jnp.dot(step, pick, preferred_element_type=F32).astype(BF16)
        for w in (gate, value, write, read, mine):
            w_pair[at, to : to + w.shape[1]] = w
            to += w.shape[1]
        w_pair_out[at, :] = out

    keep_pair(0, w_gate[1], w_value[1], w_write[1], w_read[1], w_step[1], w_out[0])
    decay_log = []
    for l in range(layers):
        decay_pad[l, 0:heads, :] = log_decay[l]
        picked = lax.dot_general(at_position, decay_pad[l], LAST, precision=HIGH, preferred_element_type=F32)
        decay_log.append(picked[0:2])
        head_pad[l, 0:1, 0:heads] = step_bias[l : l + 1, :]
        head_pad[l, 1:2, 0:heads] = jnp.exp(log_rate[l : l + 1, :])
        for taps, hist, row in (
            (taps_value, hist_value, 2),
            (taps_write, hist_write, 4),
            (taps_read, hist_read, 5),
        ):
            tap = taps[l].astype(F32)
            total = None
            for k in range(depth):
                rows = hist[l, k].astype(F32)
                valid = jnp.where(
                    lax.broadcasted_iota(jnp.int32, rows.shape, 0) == 0,
                    jnp.where(k >= depth - position[0], 1.0, 0.0),
                    jnp.where(k >= depth - position[1], 1.0, 0.0),
                )
                term = rows * tap[k : k + 1] * valid
                total = term if total is None else total + term
            for c in range(rows.shape[1] // LANES):
                for s in range(2):
                    at = s * BLOCKS + row + c
                    conv_base[l, at : at + 1, :] = total[s : s + 1, c * LANES : (c + 1) * LANES]
                    conv_last[l, at : at + 1, :] = tap[depth : depth + 1, c * LANES : (c + 1) * LANES]
    for l in range(layers):
        high = state[l].astype(BF16)
        state_hi[l] = high
        state_lo[l] = (state[l] - high.astype(F32)).astype(BF16)

    pl.semaphore_wait(barrier, n_dp - 1 + tp)

    row16 = lax.broadcasted_iota(jnp.int32, (2 * BLOCKS, LANES), 0)
    is_gate = lax.rem(row16, BLOCKS) < 2
    row_of8 = lax.broadcasted_iota(jnp.int32, (8, LANES), 0)
    assert layers == 2
    for l in range(layers):
        if l == 0:
            for o in far_first(n_dp):
                to = lax.rem(dp + o, n_dp)
                send(rs_send.at[to], rs_recv.at[dp], rs_ssem.at[l], rs_rsem.at[l], dp=to)
            rs_recv[dp] = rs_send[dp]
            for z in range(n_tp - 1):

                @pl.when(z < tp)
                def _(z=z):
                    pl.semaphore_signal(entered, inc=1, device_id={"tp": z}, device_id_type=MESH)

            swaps = (
                (w_gate.at[1], o_gate),
                (w_value.at[1], o_value),
                (w_write.at[1], o_write),
                (w_read.at[1], o_read),
                (w_step.at[1], o_step),
                (w_out.at[0], o_out),
                (in_gain, o_gain),
                (hidden, o_hidden),
            )
            for i, (src, dst) in enumerate(swaps):
                send(src, dst, swap_ssem.at[i], swap_rsem.at[i], dp=sibling)
            wait_bytes(rs_recv.at[pl.ds(0, n_dp - 1)], rs_rsem.at[l])
            received = rs_recv[...]
        else:

            @pl.when(jnp.logical_not(served_here))
            def _():
                send(
                    rs_half_send.at[my_place],
                    rs_half_recv.at[chip],
                    rs_ssem.at[1],
                    rs_rsem.at[1],
                    dp=core * chips + my_place,
                )

            @pl.when(served_here)
            def _():
                rs_half_recv[chip] = rs_half_send[my_place]

            for o in far_first(chips):
                to = lax.rem(my_place + o, chips)
                send(rs_half_send.at[to], rs_half_recv.at[chip], rs_ssem.at[l], rs_rsem.at[l], dp=core * chips + to)
            send(x_mine, x_other, swap_ssem.at[8], swap_rsem.at[8], dp=sibling)
            wait_half(rs_half_recv, rs_rsem.at[l])
            received = rs_half_recv[...]
        summed = jnp.sum(received.astype(F32), axis=0)
        rest = jnp.concatenate(
            [summed[BLOCKS * s + 6 : BLOCKS * s + 7] + summed[BLOCKS * s + 7 : BLOCKS * s + 8] for s in range(2)], axis=0
        )
        row_scale = lax.rsqrt(rest[:, heads : heads + 1] / width + epsilon)
        scale16 = jnp.where(row16 < BLOCKS, row_scale[0:1], row_scale[1:2])
        scaled = summed * scale16
        current = high_part(scaled)
        act = silu(jnp.where(is_gate, scaled, conv_base[l] + current * conv_last[l]))
        z = rest * row_scale + head_pad[l, 0:1, :]
        step = jnp.maximum(z, 0.0) + jnp.log1p(jnp.exp(-jnp.abs(z)))
        decay = jnp.exp(decay_log[l] - head_pad[l, 1:2, :] * step) * is_live
        gate_row = jnp.concatenate([lane_rows(act, BLOCKS * s) for s in range(2)], axis=0)
        value_row = jnp.concatenate([lane_rows(act, BLOCKS * s + 2) for s in range(2)], axis=0)
        step_value = per_head(step) * value_row
        decay_row = per_head(decay)
        readout, along = [], []
        for s in range(2):
            write = act[BLOCKS * s + 4 : BLOCKS * s + 5]
            read = act[BLOCKS * s + 5 : BLOCKS * s + 6]
            high = high_part(read)
            lhs = jnp.where(row_of8 == 0, high, jnp.where(row_of8 == 1, read - high, 0.0)).astype(BF16)
            a = lax.dot_general(lhs, state_hi[l, s], LAST, preferred_element_type=F32)
            b = lax.dot_general(lhs, state_lo[l, s], LAST, preferred_element_type=F32)
            readout.append(a[0:1] + a[1:2] + b[0:1])
            along.append(jnp.sum(write * read, axis=1, keepdims=True))
        readout = jnp.concatenate(readout, axis=0)
        along = jnp.concatenate(along, axis=0)
        mixed = (
            decay_row * readout + step_value * along + per_head(direct_gain[l : l + 1, :]) * value_row
        ) * gate_row
        mean = jnp.sum(mixed * mixed, axis=1, keepdims=True) / inner
        gated = mixed * lax.rsqrt(mean + epsilon) * group_gain[l : l + 1, :]
        ag_send[l] = gated.astype(BF16)
        if l == 0:
            for o in far_first(chips):
                to = 2 * lax.rem(chip + o, chips) + my_half
                send(ag_send.at[l], ag_half_recv.at[my_place], ag_ssem.at[l], ag_rsem.at[l], dp=to)

            @pl.when(jnp.logical_not(served_here))
            def _():
                send(ag_send.at[0], ag_half_recv.at[my_place], ag_ssem.at[0], ag_rsem.at[0], dp=sibling)

            @pl.when(served_here)
            def _():
                ag_half_recv[my_place] = ag_send[0]
        else:
            for d in range(n_dp):

                @pl.when(dp != d)
                def _(d=d):
                    send(ag_send.at[1], ag_recv.at[dp], ag_ssem.at[1], ag_rsem.at[1], dp=d)

            ag_recv[dp] = ag_send[l]

        for b in range(inner // LANES):
            cols = jnp.transpose(
                jnp.concatenate(
                    [step_value[:, b * LANES : (b + 1) * LANES], jnp.zeros((6, LANES), F32)], axis=0
                )
            )
            for s in range(2):
                write = act[BLOCKS * s + 4 : BLOCKS * s + 5]
                for j in range(LANES // head_dim):
                    h = b * (LANES // head_dim) + j
                    at = slice(h * head_dim, (h + 1) * head_dim)
                    state_new[l, s, at, :] = (
                        decay[s : s + 1, h : h + 1] * state[l, s, at, :]
                        + cols[j * head_dim : (j + 1) * head_dim, s : s + 1] * write
                    )
        for k in range(depth - 1):
            buf_value[l, k] = hist_value[l, k + 1]
            buf_write[l, k] = hist_write[l, k + 1]
            buf_read[l, k] = hist_read[l, k + 1]
        buf_value[l, depth - 1] = jnp.concatenate(
            [lane_rows(current, BLOCKS * s + 2) for s in range(2)], axis=0
        ).astype(BF16)
        buf_write[l, depth - 1] = jnp.concatenate(
            [current[BLOCKS * s + 4 : BLOCKS * s + 5] for s in range(2)], axis=0
        ).astype(BF16)
        buf_read[l, depth - 1] = jnp.concatenate(
            [current[BLOCKS * s + 5 : BLOCKS * s + 6] for s in range(2)], axis=0
        ).astype(BF16)

        half_rows = pl.ds(pl.multiple_of(core * half, half), half)
        if l == 0:
            for i, (src, dst) in enumerate(swaps):
                pltpu.make_async_copy(dst, dst, swap_rsem.at[i]).wait()
            keep_pair(feats, o_gate[...], o_value[...], o_write[...], o_read[...], o_step[...], o_out[...])
            pair_gain = jnp.concatenate([in_gain[1:2, :], o_gain[1:2, :]], axis=1)
            x = jnp.concatenate([hidden[half_rows, :].astype(F32), o_hidden[half_rows, :].astype(F32)], axis=1)
            wait_half(ag_half_recv, ag_rsem.at[l])
            for d in range(chips):
                gathered[2 * d : 2 * d + 2, :] = ag_half_recv[d].astype(F32)
            rows, weight = gathered[0:half, :].astype(BF16), w_pair_out[...]
        else:
            wait_bytes(x_other, swap_rsem.at[8])
            mine, other = x[:, :feats], x_other[...].astype(F32)[:, feats:]
            is_first = core == 0
            x = jnp.concatenate([jnp.where(is_first, mine, other), jnp.where(is_first, other, mine)], axis=1)
            wait_bytes(ag_recv.at[pl.ds(0, n_dp - 1)], ag_rsem.at[l])
            for d in range(n_dp):
                gathered[2 * d : 2 * d + 2, :] = ag_recv[d].astype(F32)
            rows = jnp.concatenate([gathered[0:half, :], gathered[half:, :]], axis=1).astype(BF16)
            weight = w_pack[...]
        ar_send[l] = lax.dot_general(rows, weight, LAST, preferred_element_type=F32).astype(BF16)
        if l == 0:

            @pl.when(tp < n_tp - 1)
            def _():
                pl.semaphore_wait(entered, n_tp - 1 - tp)

            for o in far_first(n_tp):
                send(ar_send.at[l], ar_recv.at[l, tp], ar_ssem.at[l], ar_rsem.at[l], tp=lax.rem(tp + o, n_tp))
            ar_recv[l, tp] = ar_send[l]
            wait_bytes(ar_recv.at[l, pl.ds(0, n_tp - 1)], ar_rsem.at[l])
            x = high_part(x + jnp.sum(ar_recv[l].astype(F32), axis=0))
            normed = (x * pair_gain).astype(BF16)
            columns = cut(jnp.dot(normed, w_pair[...], preferred_element_type=F32))
            step = columns.pop()
            rs_half_send[...] = lay_out(with_rest(columns, step, jnp.sum(x * x, axis=1, keepdims=True)), half)
            x_mine[...] = x.astype(BF16)

    giver = min(2, n_tp - 1)
    is_first_row, is_giver = tp == 0, tp == giver
    is_taker = jnp.logical_not(jnp.logical_or(is_first_row, is_giver))

    def put_out(rows):
        stream_out[...] = jnp.concatenate([rows[:, :feats], rows[:, feats:]], axis=0).astype(BF16)

    def summed_stream():
        wait_bytes(ar_recv.at[1, pl.ds(0, n_tp - 1)], ar_rsem.at[1])
        return high_part(x + jnp.sum(ar_recv[1].astype(F32), axis=0))

    for z in (0, giver):

        @pl.when(tp != z)
        def _(z=z):
            send(ar_send.at[1], ar_recv.at[1, tp], ar_ssem.at[1], ar_rsem.at[1], tp=z)

    ar_recv[1, tp] = ar_send[1]
    wait_bytes(rs_send.at[pl.ds(0, n_dp - 1)], rs_ssem.at[0])
    wait_half(rs_half_send, rs_ssem.at[1])
    wait_half(ag_half_recv, ag_ssem.at[0])
    wait_bytes(ag_recv.at[pl.ds(0, n_dp - 1)], ag_ssem.at[1])
    wait_bytes(ar_recv.at[0, pl.ds(0, n_tp - 1)], ar_ssem.at[0])
    for i, (src, dst) in enumerate(swaps):
        pltpu.make_async_copy(src, src, swap_ssem.at[i]).wait()
    wait_bytes(x_mine, swap_ssem.at[8])

    @pl.when(is_taker)
    def _():
        wait_bytes(ar_recv.at[0, pl.ds(0, 2)], ar_ssem.at[1])

    @pl.when(jnp.logical_not(is_taker))
    def _():
        wait_bytes(ar_send.at[1], ar_ssem.at[1])

    @pl.when(is_first_row)
    def _():
        put_out(summed_stream())

    @pl.when(is_giver)
    def _():
        last = summed_stream()
        x_last[...] = last.astype(BF16)
        for z in range(1, n_tp):
            if z != giver:
                send(x_last, x_given, last_ssem, last_rsem, tp=z)
        put_out(last)
        wait_bytes(ar_recv.at[1, pl.ds(0, n_tp - 2)], last_ssem)

    @pl.when(is_taker)
    def _():
        wait_bytes(x_given, last_rsem)
        put_out(x_given[...].astype(F32))


def on_device(
    hidden,
    lengths,
    input_norm_gain,
    gate_matrix,
    input_matrix,
    write_matrix,
    read_matrix,
    step_matrix,
    step_size_bias,
    log_decay_rate,
    direct_path_gain,
    input_filter_taps,
    write_filter_taps,
    read_filter_taps,
    position_log_decay,
    grouped_norm_gain,
    output_matrix,
    recurrent_head_state,
    history_input_rows,
    history_write_rows,
    history_read_rows,
):
    n_dp, n_tp = lax.axis_size("dp"), lax.axis_size("tp")
    layers, seq_local, heads, head_dim, state_dim = recurrent_head_state.shape
    inner = heads * head_dim
    seqs, feats = hidden.shape
    assert seq_local == 2 and state_dim == LANES and write_matrix.shape[2] == LANES and inner == 2 * LANES
    state_shape = (layers, seq_local, inner, state_dim)
    operands = (
        hidden,
        lengths,
        input_norm_gain,
        gate_matrix,
        input_matrix,
        write_matrix,
        read_matrix,
        step_matrix,
        step_size_bias,
        log_decay_rate,
        direct_path_gain,
        input_filter_taps,
        write_filter_taps,
        read_filter_taps,
        position_log_decay.transpose(0, 2, 1),
        grouped_norm_gain,
        output_matrix.transpose(0, 2, 1),
        recurrent_head_state.reshape(state_shape),
        history_input_rows.transpose(0, 2, 1, 3),
        history_write_rows.transpose(0, 2, 1, 3),
        history_read_rows.transpose(0, 2, 1, 3),
    )
    vmem, hbm = pl.BlockSpec(memory_space=pltpu.VMEM), pl.BlockSpec(memory_space=pltpu.HBM)
    in_specs = [hbm] * len(operands)
    results = [operands[i] for i in (0, 17, 18, 19, 20)]
    positions = position_log_decay.shape[1]
    dma = pltpu.SemaphoreType.DMA
    whole = [o for i, o in enumerate(operands) if i != 17]
    space = lambda o: pltpu.SMEM if o is lengths else pltpu.VMEM
    finished = pl.pallas_call(
        functools.partial(kernel, n_dp, n_tp),
        out_shape=[pltpu.VMEM(r.shape, r.dtype) for r in results],
        in_specs=in_specs,
        out_specs=[vmem] * len(results),
        scratch_shapes=[space(o)(o.shape, o.dtype) for o in whole]
        + [
            pltpu.VMEM((seqs * BLOCKS, LANES), F32),
            pltpu.VMEM((n_dp, 2 * BLOCKS, LANES), BF16),
            pltpu.VMEM((n_dp, 2 * BLOCKS, LANES), BF16),
            pltpu.VMEM((n_dp // 2, 2 * BLOCKS, LANES), BF16),
            pltpu.VMEM((n_dp // 2, 2 * BLOCKS, LANES), BF16),
            pltpu.VMEM((layers, 2, inner), BF16),
            pltpu.VMEM((n_dp // 2, 2, inner), BF16),
            pltpu.VMEM((n_dp, 2, inner), BF16),
            pltpu.VMEM((seqs, inner), F32),
            pltpu.VMEM((layers, seqs // 2, 2 * feats), BF16),
            pltpu.VMEM((layers, n_tp, seqs // 2, 2 * feats), BF16),
            pltpu.VMEM((2 * feats, 7 * LANES), BF16),
            pltpu.VMEM((2 * feats, inner), BF16),
            pltpu.VMEM((seqs // 2, 2 * feats), BF16),
            pltpu.VMEM((seqs // 2, 2 * feats), BF16),
            pltpu.VMEM((seqs // 2, 2 * feats), BF16),
            pltpu.VMEM((seqs // 2, 2 * feats), BF16),
            pltpu.VMEM(state_shape, F32),
            pltpu.VMEM(state_shape, BF16),
            pltpu.VMEM(state_shape, BF16),
            pltpu.VMEM((2 * feats, 2 * inner), BF16),
            pltpu.VMEM((layers, 2 * BLOCKS, LANES), F32),
            pltpu.VMEM((layers, 2 * BLOCKS, LANES), F32),
            pltpu.VMEM((layers, LANES, positions), F32),
            pltpu.VMEM((layers, 8, LANES), F32),
        ]
        + [pltpu.VMEM(o.shape[1:], o.dtype) for o in (gate_matrix, input_matrix, write_matrix, read_matrix, step_matrix)]
        + [
            pltpu.VMEM(operands[16].shape[1:], BF16),
            pltpu.VMEM(input_norm_gain.shape, F32),
            pltpu.VMEM(hidden.shape, BF16),
            dma((9,)),
            dma((9,)),
        ]
        + [dma((layers,))] * 6
        + [pltpu.SemaphoreType.REGULAR, dma, dma]
        + [dma((len(whole) + 1,))],
        compiler_params=pltpu.CompilerParams(
            collective_id=0, has_side_effects=True
        ),
        name="mixers",
    )(*operands)
    stream, states, values, writes, reads = pl.pallas_call(
        flush,
        out_shape=[jax.ShapeDtypeStruct(r.shape, r.dtype) for r in results],
        in_specs=[vmem] * len(results),
        out_specs=[hbm] * len(results),
        scratch_shapes=[dma((len(results),))],
        compiler_params=pltpu.CompilerParams(vmem_limit_bytes=4 * 1024 * 1024),
        name="flush",
    )(*finished)
    return (
        stream,
        states.reshape(recurrent_head_state.shape),
        values.transpose(0, 2, 1, 3),
        writes.transpose(0, 2, 1, 3),
        reads.transpose(0, 2, 1, 3),
    )


def solution(mesh):
    placed = (
        P("grp", "dp"),
        P(("grp", "dp")),
        P(None, "dp"),
        P(None, "dp", "tp"),
        P(None, "dp", "tp"),
        P(None, "dp", "tp"),
        P(None, "dp", "tp"),
        P(None, "dp", None),
        P(None, "tp"),
        P(None, "tp"),
        P(None, "tp"),
        P(None, None, "tp"),
        P(None, None, "tp"),
        P(None, None, "tp"),
        P(None, None, "tp"),
        P(None, "tp"),
        P(None, "tp", "dp"),
        P(None, ("grp", "dp"), "tp", None, None),
        P(None, ("grp", "dp"), None, "tp"),
        P(None, ("grp", "dp"), None, "tp"),
        P(None, ("grp", "dp"), None, "tp"),
    )
    return jax.shard_map(
        on_device,
        mesh=mesh,
        in_specs=placed,
        out_specs=(
            P("grp", "dp"),
            P(None, ("grp", "dp"), "tp", None, None),
            P(None, ("grp", "dp"), None, "tp"),
            P(None, ("grp", "dp"), None, "tp"),
            P(None, ("grp", "dp"), None, "tp"),
        ),
        check_vma=False,
    )
```

```python
import functools

import jax
import jax.numpy as jnp
from jax import lax
from jax.experimental import pallas as pl
from jax.experimental.pallas import tpu as pltpu
from jax.sharding import PartitionSpec as P

MESH = pl.DeviceIdType.MESH
F32 = jnp.float32
BF16 = jnp.bfloat16
epsilon = 1e-06
LANES = 128
BLOCKS = 8
HIGH = lax.Precision.HIGHEST
LAST = (((1,), (1,)), ((), ()))


def far_first(count):
    return sorted(range(1, count), key=lambda o: -min(o, count - o))


def silu(z):
    return z / (1.0 + jnp.exp(-z))


def high_part(v):
    return v.astype(BF16).astype(F32)


def wait_bytes(ref, sem):
    pltpu.make_async_copy(ref, ref, sem).wait()


def lane_rows(block, first):
    return jnp.concatenate([block[first : first + 1], block[first + 1 : first + 2]], axis=1)


def flush(*refs):
    count = len(refs) // 2
    sems = refs[-1]
    copies = [pltpu.make_async_copy(refs[i], refs[count + i], sems.at[i]) for i in range(count)]
    for c in copies:
        c.start()
    for c in copies:
        c.wait()


def kernel(n_dp, n_tp, *refs):
    given, rest = refs[:21], refs[21:]
    outs, held, rest = rest[:5], rest[5:25], rest[25:]
    scratch, in_sem = rest[:-1], rest[-1]
    state_in = given[17]
    whole = [g for i, g in enumerate(given) if i != 17]
    barrier = pltpu.get_barrier_semaphore()
    dp, tp = lax.axis_index("dp"), lax.axis_index("tp")
    state = scratch[17]
    loads = [pltpu.make_async_copy(g, h, in_sem.at[i]) for i, (g, h) in enumerate(zip(whole, held))]
    loads.append(pltpu.make_async_copy(state_in, state, in_sem.at[len(whole)]))
    for c in loads[:9]:
        c.start()
    for o in far_first(n_dp):
        pl.semaphore_signal(barrier, inc=1, device_id={"dp": lax.rem(dp + o, n_dp)}, device_id_type=MESH)
    for c in loads[9:]:
        c.start()
    for z in range(n_tp - 1, 0, -1):

        @pl.when(z > tp)
        def _(z=z):
            pl.semaphore_signal(barrier, inc=1, device_id={"tp": z}, device_id_type=MESH)

    body(n_dp, n_tp, barrier, loads, *held, *outs, *scratch)


def body(
    n_dp,
    n_tp,
    barrier,
    loads,
    hidden,
    lengths,
    in_gain,
    w_gate,
    w_value,
    w_write,
    w_read,
    w_step,
    step_bias,
    log_rate,
    direct_gain,
    taps_value,
    taps_write,
    taps_read,
    log_decay,
    group_gain,
    w_out,
    hist_value,
    hist_write,
    hist_read,
    stream_out,
    state_new,
    buf_value,
    buf_write,
    buf_read,
    part,
    rs_send,
    rs_recv,
    rs_half_send,
    rs_half_recv,
    ag_send,
    ag_half_recv,
    ag_recv,
    gathered,
    ar_send,
    ar_recv,
    w_pair,
    w_pair_out,
    x_mine,
    x_other,
    x_last,
    x_given,
    state,
    state_hi,
    state_lo,
    w_pack,
    conv_base,
    conv_last,
    decay_pad,
    head_pad,
    o_gate,
    o_value,
    o_write,
    o_read,
    o_step,
    o_out,
    o_gain,
    o_hidden,
    swap_ssem,
    swap_rsem,
    rs_ssem,
    rs_rsem,
    ag_ssem,
    ag_rsem,
    ar_ssem,
    ar_rsem,
    entered,
    last_ssem,
    last_rsem,
):
    dp, tp = lax.axis_index("dp"), lax.axis_index("tp")
    layers, feats = in_gain.shape
    seqs = hidden.shape[0]
    width = feats * n_dp
    heads = step_bias.shape[1]
    inner = w_gate.shape[2]
    head_dim = inner // heads
    depth = hist_value.shape[1]
    half = seqs // 2

    lane_inner = lax.broadcasted_iota(jnp.int32, (2, inner), 1)
    pick = (
        lax.broadcasted_iota(jnp.int32, (w_step.shape[2], LANES), 0)
        == lax.broadcasted_iota(jnp.int32, (w_step.shape[2], LANES), 1) + tp * heads
    ) & (lax.broadcasted_iota(jnp.int32, (w_step.shape[2], LANES), 1) < heads)
    pick = pick.astype(F32).astype(BF16)

    def per_head(rows):
        out = jnp.broadcast_to(rows[:, heads - 1 : heads], (rows.shape[0], inner))
        lane = lane_inner[: rows.shape[0]]
        for h in range(heads - 2, -1, -1):
            out = jnp.where(lane < (h + 1) * head_dim, rows[:, h : h + 1], out)
        return out

    def lay_out(columns, count):
        for c, column in enumerate(columns):
            part[pl.ds(c, count, stride=BLOCKS), :] = column
        return part[0 : count * BLOCKS, :].reshape(count // 2, 2 * BLOCKS, LANES).astype(BF16)

    def with_rest(columns, step, square):
        lane = lax.broadcasted_iota(jnp.int32, step.shape, 1)
        rest = jnp.where(lane == heads, square, step)
        high = high_part(rest)
        return columns + [high, rest - high]

    def cut(r):
        return [r[:, at : at + LANES] for at in range(0, r.shape[1], LANES)]

    def send(src, dst, ssem, rsem, **to):
        pltpu.make_async_remote_copy(
            src_ref=src, dst_ref=dst, send_sem=ssem, recv_sem=rsem, device_id=to, device_id_type=MESH
        ).start()

    chip, core = dp // 2, lax.rem(dp, 2)
    chips = n_dp // 2
    sibling = dp + 1 - 2 * core
    my_half, my_place = dp // chips, lax.rem(dp, chips)
    served_here = my_half == core

    def wait_half(ref, sem):
        @pl.when(served_here)
        def _():
            wait_bytes(ref.at[pl.ds(0, chips - 1)], sem)

        @pl.when(jnp.logical_not(served_here))
        def _():
            wait_bytes(ref, sem)


    for c in loads[:8]:
        c.wait()
    x_bf = hidden[...]
    x = x_bf.astype(F32)
    normed = (x * in_gain[0:1, :]).astype(BF16)
    columns = []
    for w in (w_gate, w_value, w_write, w_read):
        columns += cut(jnp.dot(normed, w[0], preferred_element_type=F32))
    w_mine = jnp.dot(w_step[0], pick, preferred_element_type=F32).astype(BF16)
    step = jnp.dot(normed, w_mine, preferred_element_type=F32)
    rs_send[...] = lay_out(with_rest(columns, step, jnp.sum(x * x, axis=1, keepdims=True)), seqs)

    for c in loads[8:]:
        c.wait()
    position = [lengths[s] - 1 for s in range(2)]
    row8 = lax.broadcasted_iota(jnp.int32, (8, log_decay.shape[2]), 0)
    lane_pos = lax.broadcasted_iota(jnp.int32, (8, log_decay.shape[2]), 1)
    at_position = (lane_pos == jnp.where(row8 == 0, position[0], position[1])).astype(F32)
    row2 = lax.broadcasted_iota(jnp.int32, (2, LANES), 0)
    is_live = jnp.where(jnp.where(row2 == 0, position[0], position[1]) > 0, 1.0, 0.0)
    conv_base[...] = jnp.zeros_like(conv_base)
    conv_last[...] = jnp.zeros_like(conv_last)
    decay_pad[...] = jnp.zeros_like(decay_pad)
    head_pad[...] = jnp.zeros_like(head_pad)
    w_pack[...] = jnp.zeros_like(w_pack)
    w_pack[0:feats, 0:inner] = w_out[1]
    w_pack[feats : 2 * feats, inner : 2 * inner] = w_out[1]

    def keep_pair(first, gate, value, write, read, step, out):
        at, to = slice(first, first + feats), 0
        mine = jnp.dot(step, pick, preferred_element_type=F32).astype(BF16)
        for w in (gate, value, write, read, mine):
            w_pair[at, to : to + w.shape[1]] = w
            to += w.shape[1]
        w_pair_out[at, :] = out

    keep_pair(0, w_gate[1], w_value[1], w_write[1], w_read[1], w_step[1], w_out[0])
    decay_log = []
    for l in range(layers):
        decay_pad[l, 0:heads, :] = log_decay[l]
        picked = lax.dot_general(at_position, decay_pad[l], LAST, precision=HIGH, preferred_element_type=F32)
        decay_log.append(picked[0:2])
        head_pad[l, 0:1, 0:heads] = step_bias[l : l + 1, :]
        head_pad[l, 1:2, 0:heads] = jnp.exp(log_rate[l : l + 1, :])
        for taps, hist, row in (
            (taps_value, hist_value, 2),
            (taps_write, hist_write, 4),
            (taps_read, hist_read, 5),
        ):
            tap = taps[l].astype(F32)
            total = None
            for k in range(depth):
                rows = hist[l, k].astype(F32)
                valid = jnp.where(
                    lax.broadcasted_iota(jnp.int32, rows.shape, 0) == 0,
                    jnp.where(k >= depth - position[0], 1.0, 0.0),
                    jnp.where(k >= depth - position[1], 1.0, 0.0),
                )
                term = rows * tap[k : k + 1] * valid
                total = term if total is None else total + term
            for c in range(rows.shape[1] // LANES):
                for s in range(2):
                    at = s * BLOCKS + row + c
                    conv_base[l, at : at + 1, :] = total[s : s + 1, c * LANES : (c + 1) * LANES]
                    conv_last[l, at : at + 1, :] = tap[depth : depth + 1, c * LANES : (c + 1) * LANES]
    for l in range(layers):
        high = state[l].astype(BF16)
        state_hi[l] = high
        state_lo[l] = (state[l] - high.astype(F32)).astype(BF16)

    pl.semaphore_wait(barrier, n_dp - 1 + tp)

    row16 = lax.broadcasted_iota(jnp.int32, (2 * BLOCKS, LANES), 0)
    is_gate = lax.rem(row16, BLOCKS) < 2
    row_of8 = lax.broadcasted_iota(jnp.int32, (8, LANES), 0)
    assert layers == 2
    for l in range(layers):
        if l == 0:
            for o in far_first(n_dp):
                to = lax.rem(dp + o, n_dp)
                send(rs_send.at[to], rs_recv.at[dp], rs_ssem.at[l], rs_rsem.at[l], dp=to)
            rs_recv[dp] = rs_send[dp]
            for z in range(n_tp - 1):

                @pl.when(z < tp)
                def _(z=z):
                    pl.semaphore_signal(entered, inc=1, device_id={"tp": z}, device_id_type=MESH)

            swaps = (
                (w_gate.at[1], o_gate),
                (w_value.at[1], o_value),
                (w_write.at[1], o_write),
                (w_read.at[1], o_read),
                (w_step.at[1], o_step),
                (w_out.at[0], o_out),
                (in_gain, o_gain),
                (hidden, o_hidden),
            )
            wait_bytes(rs_recv.at[pl.ds(0, n_dp - 1)], rs_rsem.at[l])
            received = rs_recv[...]
        else:

            crossed = lax.rem(my_half + core, 2) * (chips // 2)
            for o in far_first(chips):
                to = lax.rem(my_place + o + crossed, chips)
                send(rs_half_send.at[to], rs_half_recv.at[chip], rs_ssem.at[l], rs_rsem.at[l], dp=core * chips + to)

            @pl.when(jnp.logical_not(served_here))
            def _():
                to = lax.rem(my_place + chips // 2, chips)
                send(rs_half_send.at[to], rs_half_recv.at[chip], rs_ssem.at[1], rs_rsem.at[1], dp=core * chips + to)

            @pl.when(served_here)
            def _():
                rs_half_recv[chip] = rs_half_send[my_place]

            send(x_mine, x_other, swap_ssem.at[8], swap_rsem.at[8], dp=sibling)
            wait_half(rs_half_recv, rs_rsem.at[l])
            received = rs_half_recv[...]
        summed = jnp.sum(received.astype(F32), axis=0)
        rest = jnp.concatenate(
            [summed[BLOCKS * s + 6 : BLOCKS * s + 7] + summed[BLOCKS * s + 7 : BLOCKS * s + 8] for s in range(2)], axis=0
        )
        row_scale = lax.rsqrt(rest[:, heads : heads + 1] / width + epsilon)
        scale16 = jnp.where(row16 < BLOCKS, row_scale[0:1], row_scale[1:2])
        scaled = summed * scale16
        current = high_part(scaled)
        act = silu(jnp.where(is_gate, scaled, conv_base[l] + current * conv_last[l]))
        z = rest * row_scale + head_pad[l, 0:1, :]
        step = jnp.maximum(z, 0.0) + jnp.log1p(jnp.exp(-jnp.abs(z)))
        decay = jnp.exp(decay_log[l] - head_pad[l, 1:2, :] * step) * is_live
        gate_row = jnp.concatenate([lane_rows(act, BLOCKS * s) for s in range(2)], axis=0)
        value_row = jnp.concatenate([lane_rows(act, BLOCKS * s + 2) for s in range(2)], axis=0)
        step_value = per_head(step) * value_row
        decay_row = per_head(decay)
        readout, along = [], []
        for s in range(2):
            write = act[BLOCKS * s + 4 : BLOCKS * s + 5]
            read = act[BLOCKS * s + 5 : BLOCKS * s + 6]
            high = high_part(read)
            lhs = jnp.where(row_of8 == 0, high, jnp.where(row_of8 == 1, read - high, 0.0)).astype(BF16)
            a = lax.dot_general(lhs, state_hi[l, s], LAST, preferred_element_type=F32)
            b = lax.dot_general(lhs, state_lo[l, s], LAST, preferred_element_type=F32)
            readout.append(a[0:1] + a[1:2] + b[0:1])
            along.append(jnp.sum(write * read, axis=1, keepdims=True))
        readout = jnp.concatenate(readout, axis=0)
        along = jnp.concatenate(along, axis=0)
        mixed = (
            decay_row * readout + step_value * along + per_head(direct_gain[l : l + 1, :]) * value_row
        ) * gate_row
        mean = jnp.sum(mixed * mixed, axis=1, keepdims=True) / inner
        gated = mixed * lax.rsqrt(mean + epsilon) * group_gain[l : l + 1, :]
        ag_send[l] = gated.astype(BF16)
        if l == 0:
            for o in far_first(chips):
                to = 2 * lax.rem(chip + o, chips) + my_half
                send(ag_send.at[l], ag_half_recv.at[my_place], ag_ssem.at[l], ag_rsem.at[l], dp=to)

            @pl.when(jnp.logical_not(served_here))
            def _():
                send(ag_send.at[0], ag_half_recv.at[my_place], ag_ssem.at[0], ag_rsem.at[0], dp=sibling)

            @pl.when(served_here)
            def _():
                ag_half_recv[my_place] = ag_send[0]

            for i, (src, dst) in enumerate(swaps):
                send(src, dst, swap_ssem.at[i], swap_rsem.at[i], dp=sibling)
        else:
            for d in range(n_dp):

                @pl.when(dp != d)
                def _(d=d):
                    send(ag_send.at[1], ag_recv.at[dp], ag_ssem.at[1], ag_rsem.at[1], dp=d)

            ag_recv[dp] = ag_send[l]

        for b in range(inner // LANES):
            cols = jnp.transpose(
                jnp.concatenate(
                    [step_value[:, b * LANES : (b + 1) * LANES], jnp.zeros((6, LANES), F32)], axis=0
                )
            )
            for s in range(2):
                write = act[BLOCKS * s + 4 : BLOCKS * s + 5]
                for j in range(LANES // head_dim):
                    h = b * (LANES // head_dim) + j
                    at = slice(h * head_dim, (h + 1) * head_dim)
                    state_new[l, s, at, :] = (
                        decay[s : s + 1, h : h + 1] * state[l, s, at, :]
                        + cols[j * head_dim : (j + 1) * head_dim, s : s + 1] * write
                    )
        for k in range(depth - 1):
            buf_value[l, k] = hist_value[l, k + 1]
            buf_write[l, k] = hist_write[l, k + 1]
            buf_read[l, k] = hist_read[l, k + 1]
        buf_value[l, depth - 1] = jnp.concatenate(
            [lane_rows(current, BLOCKS * s + 2) for s in range(2)], axis=0
        ).astype(BF16)
        buf_write[l, depth - 1] = jnp.concatenate(
            [current[BLOCKS * s + 4 : BLOCKS * s + 5] for s in range(2)], axis=0
        ).astype(BF16)
        buf_read[l, depth - 1] = jnp.concatenate(
            [current[BLOCKS * s + 5 : BLOCKS * s + 6] for s in range(2)], axis=0
        ).astype(BF16)

        half_rows = pl.ds(pl.multiple_of(core * half, half), half)
        if l == 0:
            for i, (src, dst) in enumerate(swaps):
                pltpu.make_async_copy(dst, dst, swap_rsem.at[i]).wait()
            keep_pair(feats, o_gate[...], o_value[...], o_write[...], o_read[...], o_step[...], o_out[...])
            pair_gain = jnp.concatenate([in_gain[1:2, :], o_gain[1:2, :]], axis=1)
            x = jnp.concatenate([hidden[half_rows, :].astype(F32), o_hidden[half_rows, :].astype(F32)], axis=1)
            wait_half(ag_half_recv, ag_rsem.at[l])
            for d in range(chips):
                gathered[2 * d : 2 * d + 2, :] = ag_half_recv[d].astype(F32)
            rows, weight = gathered[0:half, :].astype(BF16), w_pair_out[...]
        else:
            wait_bytes(x_other, swap_rsem.at[8])
            mine, other = x[:, :feats], x_other[...].astype(F32)[:, feats:]
            is_first = core == 0
            x = jnp.concatenate([jnp.where(is_first, mine, other), jnp.where(is_first, other, mine)], axis=1)
            wait_bytes(ag_recv.at[pl.ds(0, n_dp - 1)], ag_rsem.at[l])
            for d in range(n_dp):
                gathered[2 * d : 2 * d + 2, :] = ag_recv[d].astype(F32)
            rows = jnp.concatenate([gathered[0:half, :], gathered[half:, :]], axis=1).astype(BF16)
            weight = w_pack[...]
        ar_send[l] = lax.dot_general(rows, weight, LAST, preferred_element_type=F32).astype(BF16)
        if l == 0:

            @pl.when(tp < n_tp - 1)
            def _():
                pl.semaphore_wait(entered, n_tp - 1 - tp)

            for o in far_first(n_tp):
                send(ar_send.at[l], ar_recv.at[l, tp], ar_ssem.at[l], ar_rsem.at[l], tp=lax.rem(tp + o, n_tp))
            ar_recv[l, tp] = ar_send[l]
            wait_bytes(ar_recv.at[l, pl.ds(0, n_tp - 1)], ar_rsem.at[l])
            x = high_part(x + jnp.sum(ar_recv[l].astype(F32), axis=0))
            normed = (x * pair_gain).astype(BF16)
            columns = cut(jnp.dot(normed, w_pair[...], preferred_element_type=F32))
            step = columns.pop()
            rs_half_send[...] = lay_out(with_rest(columns, step, jnp.sum(x * x, axis=1, keepdims=True)), half)
            x_mine[...] = x.astype(BF16)

    giver = min(2, n_tp - 1)
    is_first_row, is_giver = tp == 0, tp == giver
    is_taker = jnp.logical_not(jnp.logical_or(is_first_row, is_giver))

    def put_out(rows):
        stream_out[...] = jnp.concatenate([rows[:, :feats], rows[:, feats:]], axis=0).astype(BF16)

    def summed_stream():
        wait_bytes(ar_recv.at[1, pl.ds(0, n_tp - 1)], ar_rsem.at[1])
        return high_part(x + jnp.sum(ar_recv[1].astype(F32), axis=0))

    for z in (0, giver):

        @pl.when(tp != z)
        def _(z=z):
            send(ar_send.at[1], ar_recv.at[1, tp], ar_ssem.at[1], ar_rsem.at[1], tp=z)

    ar_recv[1, tp] = ar_send[1]
    wait_bytes(rs_send.at[pl.ds(0, n_dp - 1)], rs_ssem.at[0])
    wait_half(rs_half_send, rs_ssem.at[1])
    wait_half(ag_half_recv, ag_ssem.at[0])
    wait_bytes(ag_recv.at[pl.ds(0, n_dp - 1)], ag_ssem.at[1])
    wait_bytes(ar_recv.at[0, pl.ds(0, n_tp - 1)], ar_ssem.at[0])
    for i, (src, dst) in enumerate(swaps):
        pltpu.make_async_copy(src, src, swap_ssem.at[i]).wait()
    wait_bytes(x_mine, swap_ssem.at[8])

    @pl.when(is_taker)
    def _():
        wait_bytes(ar_recv.at[0, pl.ds(0, 2)], ar_ssem.at[1])

    @pl.when(jnp.logical_not(is_taker))
    def _():
        wait_bytes(ar_send.at[1], ar_ssem.at[1])

    @pl.when(is_first_row)
    def _():
        put_out(summed_stream())

    @pl.when(is_giver)
    def _():
        last = summed_stream()
        x_last[...] = last.astype(BF16)
        for z in range(1, n_tp):
            if z != giver:
                send(x_last, x_given, last_ssem, last_rsem, tp=z)
        put_out(last)
        wait_bytes(ar_recv.at[1, pl.ds(0, n_tp - 2)], last_ssem)

    @pl.when(is_taker)
    def _():
        wait_bytes(x_given, last_rsem)
        put_out(x_given[...].astype(F32))


def on_device(
    hidden,
    lengths,
    input_norm_gain,
    gate_matrix,
    input_matrix,
    write_matrix,
    read_matrix,
    step_matrix,
    step_size_bias,
    log_decay_rate,
    direct_path_gain,
    input_filter_taps,
    write_filter_taps,
    read_filter_taps,
    position_log_decay,
    grouped_norm_gain,
    output_matrix,
    recurrent_head_state,
    history_input_rows,
    history_write_rows,
    history_read_rows,
):
    n_dp, n_tp = lax.axis_size("dp"), lax.axis_size("tp")
    layers, seq_local, heads, head_dim, state_dim = recurrent_head_state.shape
    inner = heads * head_dim
    seqs, feats = hidden.shape
    assert seq_local == 2 and state_dim == LANES and write_matrix.shape[2] == LANES and inner == 2 * LANES
    state_shape = (layers, seq_local, inner, state_dim)
    operands = (
        hidden,
        lengths,
        input_norm_gain,
        gate_matrix,
        input_matrix,
        write_matrix,
        read_matrix,
        step_matrix,
        step_size_bias,
        log_decay_rate,
        direct_path_gain,
        input_filter_taps,
        write_filter_taps,
        read_filter_taps,
        position_log_decay.transpose(0, 2, 1),
        grouped_norm_gain,
        output_matrix.transpose(0, 2, 1),
        recurrent_head_state.reshape(state_shape),
        history_input_rows.transpose(0, 2, 1, 3),
        history_write_rows.transpose(0, 2, 1, 3),
        history_read_rows.transpose(0, 2, 1, 3),
    )
    vmem, hbm = pl.BlockSpec(memory_space=pltpu.VMEM), pl.BlockSpec(memory_space=pltpu.HBM)
    in_specs = [hbm] * len(operands)
    results = [operands[i] for i in (0, 17, 18, 19, 20)]
    positions = position_log_decay.shape[1]
    dma = pltpu.SemaphoreType.DMA
    whole = [o for i, o in enumerate(operands) if i != 17]
    space = lambda o: pltpu.SMEM if o is lengths else pltpu.VMEM
    finished = pl.pallas_call(
        functools.partial(kernel, n_dp, n_tp),
        out_shape=[pltpu.VMEM(r.shape, r.dtype) for r in results],
        in_specs=in_specs,
        out_specs=[vmem] * len(results),
        scratch_shapes=[space(o)(o.shape, o.dtype) for o in whole]
        + [
            pltpu.VMEM((seqs * BLOCKS, LANES), F32),
            pltpu.VMEM((n_dp, 2 * BLOCKS, LANES), BF16),
            pltpu.VMEM((n_dp, 2 * BLOCKS, LANES), BF16),
            pltpu.VMEM((n_dp // 2, 2 * BLOCKS, LANES), BF16),
            pltpu.VMEM((n_dp // 2, 2 * BLOCKS, LANES), BF16),
            pltpu.VMEM((layers, 2, inner), BF16),
            pltpu.VMEM((n_dp // 2, 2, inner), BF16),
            pltpu.VMEM((n_dp, 2, inner), BF16),
            pltpu.VMEM((seqs, inner), F32),
            pltpu.VMEM((layers, seqs // 2, 2 * feats), BF16),
            pltpu.VMEM((layers, n_tp, seqs // 2, 2 * feats), BF16),
            pltpu.VMEM((2 * feats, 7 * LANES), BF16),
            pltpu.VMEM((2 * feats, inner), BF16),
            pltpu.VMEM((seqs // 2, 2 * feats), BF16),
            pltpu.VMEM((seqs // 2, 2 * feats), BF16),
            pltpu.VMEM((seqs // 2, 2 * feats), BF16),
            pltpu.VMEM((seqs // 2, 2 * feats), BF16),
            pltpu.VMEM(state_shape, F32),
            pltpu.VMEM(state_shape, BF16),
            pltpu.VMEM(state_shape, BF16),
            pltpu.VMEM((2 * feats, 2 * inner), BF16),
            pltpu.VMEM((layers, 2 * BLOCKS, LANES), F32),
            pltpu.VMEM((layers, 2 * BLOCKS, LANES), F32),
            pltpu.VMEM((layers, LANES, positions), F32),
            pltpu.VMEM((layers, 8, LANES), F32),
        ]
        + [pltpu.VMEM(o.shape[1:], o.dtype) for o in (gate_matrix, input_matrix, write_matrix, read_matrix, step_matrix)]
        + [
            pltpu.VMEM(operands[16].shape[1:], BF16),
            pltpu.VMEM(input_norm_gain.shape, F32),
            pltpu.VMEM(hidden.shape, BF16),
            dma((9,)),
            dma((9,)),
        ]
        + [dma((layers,))] * 6
        + [pltpu.SemaphoreType.REGULAR, dma, dma]
        + [dma((len(whole) + 1,))],
        compiler_params=pltpu.CompilerParams(
            collective_id=0, has_side_effects=True
        ),
        name="mixers",
    )(*operands)
    stream, states, values, writes, reads = pl.pallas_call(
        flush,
        out_shape=[jax.ShapeDtypeStruct(r.shape, r.dtype) for r in results],
        in_specs=[vmem] * len(results),
        out_specs=[hbm] * len(results),
        scratch_shapes=[dma((len(results),))],
        compiler_params=pltpu.CompilerParams(vmem_limit_bytes=4 * 1024 * 1024),
        name="flush",
    )(*finished)
    return (
        stream,
        states.reshape(recurrent_head_state.shape),
        values.transpose(0, 2, 1, 3),
        writes.transpose(0, 2, 1, 3),
        reads.transpose(0, 2, 1, 3),
    )


def solution(mesh):
    placed = (
        P("grp", "dp"),
        P(("grp", "dp")),
        P(None, "dp"),
        P(None, "dp", "tp"),
        P(None, "dp", "tp"),
        P(None, "dp", "tp"),
        P(None, "dp", "tp"),
        P(None, "dp", None),
        P(None, "tp"),
        P(None, "tp"),
        P(None, "tp"),
        P(None, None, "tp"),
        P(None, None, "tp"),
        P(None, None, "tp"),
        P(None, None, "tp"),
        P(None, "tp"),
        P(None, "tp", "dp"),
        P(None, ("grp", "dp"), "tp", None, None),
        P(None, ("grp", "dp"), None, "tp"),
        P(None, ("grp", "dp"), None, "tp"),
        P(None, ("grp", "dp"), None, "tp"),
    )
    return jax.shard_map(
        on_device,
        mesh=mesh,
        in_specs=placed,
        out_specs=(
            P("grp", "dp"),
            P(None, ("grp", "dp"), "tp", None, None),
            P(None, ("grp", "dp"), None, "tp"),
            P(None, ("grp", "dp"), None, "tp"),
            P(None, ("grp", "dp"), None, "tp"),
        ),
        check_vma=False,
    )
```
